32 devices in a mesh: sp: 16 (over z, y, x), tp: 2 (over core).
Axes of the slice: x: 2, y: 2, z: 4, core: 2. Of those that a mesh axis runs over, the one named last changes fastest.
Arguments:
- residual: bfloat16 [3072, 2048], P(('sp', 'tp')), may hold values from -6 to 6
- queries_narrow: bfloat16 [3072, 512], P('sp', 'tp'), may hold values from -24 to 24
- keys_narrow: bfloat16 [3072, 512], P('sp', 'tp'), may hold values from -24 to 24
- values_narrow: bfloat16 [3072, 512], P('sp', 'tp'), may hold values from -6 to 6
- queries_broad: bfloat16 [3072, 512], P('sp', 'tp'), may hold values from -24 to 24
- keys_broad: bfloat16 [3072, 512], P('sp', 'tp'), may hold values from -24 to 24
- values_broad: bfloat16 [3072, 512], P('sp', 'tp'), may hold values from -6 to 6
- gates_narrow: float32 [3072, 16], P('sp', 'tp'), may hold values from -3072 to 0, as said below
- gates_broad: float32 [3072, 8], P('sp', 'tp'), may hold values from -3072 to 0, as said below
- project_narrow: bfloat16 [512, 2048], P('tp'), may hold values from -0.5 to 0.5
- project_broad: bfloat16 [512, 2048], P('tp'), may hold values from -0.5 to 0.5
- norm_gain: float32 [2048], replicated, may hold values from 0.1 to 1.9
- up_weight: bfloat16 [2048, 8192], P('sp', 'tp'), may hold values from -0.125 to 0.125
- down_weight: bfloat16 [8192, 2048], P('tp', 'sp'), may hold values from -0.0625 to 0.0625
Outputs:
- layer_out: bfloat16 [3072, 2048], P(('sp', 'tp'))
The draws below stay inside these ranges and needn't reach their ends.
Inputs may be any that keep to these rules, and one draw needn't show every extreme that they name: `gates_narrow`: each head's cumulative log gate never rises from one position to the next. `gates_broad`: each head's cumulative log gate never rises from one position to the next.
All inputs are finite; a program needn't handle non-finite values.
Results may differ from the reference program's by a relative error of at most 0.018.
Values may be sent and summed in bfloat16 or wider, within the bound.
A program may use at most 128 MiB of HBM per device.

```python
import jax
import jax.numpy as jnp
from jax import lax

D = 2048
FF = 8192
A_HEADS = 16
A_DIM = 32
B_HEADS = 8
B_DIM = 64
TOK_DEV = 192
CONTEXT_LENGTH = 3072


def paired_rows(key, width):
    key_query, key_keys = jax.random.split(key, 2)
    queries = jax.random.normal(key_query, (CONTEXT_LENGTH, width), jnp.float32)
    keys = jax.random.normal(key_keys, (CONTEXT_LENGTH, width), jnp.float32)
    return (queries.astype(jnp.bfloat16), keys.astype(jnp.bfloat16))


def draw_queries_narrow(key, part):
    return paired_rows(jax.random.fold_in(key, 11), A_HEADS * A_DIM)[0]


def draw_keys_narrow(key, part):
    return paired_rows(jax.random.fold_in(key, 11), A_HEADS * A_DIM)[1]


def draw_queries_broad(key, part):
    return paired_rows(jax.random.fold_in(key, 12), B_HEADS * B_DIM)[0]


def draw_keys_broad(key, part):
    return paired_rows(jax.random.fold_in(key, 12), B_HEADS * B_DIM)[1]


def forget_gates(key, heads):
    category_seed, quick_decay_seed, gradual_decay_seed, tile_seed, sample_seed, spike_seed, quantity_seed = jax.random.split(key, 7)
    slow_share = 0.5
    slow = jax.random.uniform(category_seed, (heads,), jnp.float32) < slow_share
    fast_rate = 1.0 / jax.random.uniform(quick_decay_seed, (heads,), jnp.float32, 30.0, 50.0)
    slow_rate = jax.random.uniform(gradual_decay_seed, (heads,), jnp.float32, 0.5, 1.0) / CONTEXT_LENGTH
    rate = jnp.where(slow, slow_rate, fast_rate)
    blocks = CONTEXT_LENGTH // TOK_DEV
    block_factor = jnp.exp(jax.random.uniform(tile_seed, (blocks,), jnp.float32, -0.7, 0.7))
    block_factor = jnp.repeat(block_factor, TOK_DEV)
    data_part = jnp.exp(jax.random.uniform(sample_seed, (CONTEXT_LENGTH, heads), jnp.float32, -1.2, 1.1))
    forget_log_factor = -rate[None, :] * block_factor[:, None] * data_part
    position_spike = jax.random.uniform(spike_seed, (CONTEXT_LENGTH, 1), jnp.float32) < 2.0 / CONTEXT_LENGTH
    position_quantity = jax.random.uniform(quantity_seed, (CONTEXT_LENGTH, heads), jnp.float32, 0.22, 0.69)
    forget_log_factor = forget_log_factor - jnp.where(position_spike, position_quantity, 0.0)
    return jnp.cumsum(forget_log_factor, axis=0)


def draw_gates_narrow(key, part):
    return forget_gates(jax.random.fold_in(key, 21), A_HEADS)


def draw_gates_broad(key, part):
    return forget_gates(jax.random.fold_in(key, 22), B_HEADS)


def block_scale(key, shape, cuts, low, high):
    gain, own = 1.0, jax.random.fold_in(key, 6)
    for dim, blocks in cuts:
        steps = jnp.exp(jax.random.uniform(jax.random.fold_in(own, dim), (blocks,), jnp.float32, low / len(cuts), high / len(cuts)))
        gain = gain * jnp.repeat(steps, shape[dim] // blocks).reshape([-1 if axis == dim else 1 for axis in range(len(shape))])
    return gain


def bell_draw(own_key, extent, spread, limit, cuts=(), kind=jnp.bfloat16):
    array = spread * jax.random.normal(own_key, extent, jnp.float32)
    if cuts:
        array = array * block_scale(own_key, extent, cuts, -0.22, 0.18)
    return jnp.clip(array, -limit, limit).astype(kind)


def setup_inputs(seed: int = 0) -> dict:
    streams_of = jax.random.split(jax.random.key(seed), 15)
    return {
        "residual": bell_draw(streams_of[0], (CONTEXT_LENGTH, D), 1.0, 6.0, ((0, 32),)),
        "queries_narrow": draw_queries_narrow(jax.random.fold_in(streams_of[14], 71), 0),
        "keys_narrow": draw_keys_narrow(jax.random.fold_in(streams_of[14], 71), 0),
        "values_narrow": bell_draw(streams_of[3], (CONTEXT_LENGTH, A_HEADS * A_DIM), 1.0, 6.0, ((0, 16), (1, 2))),
        "queries_broad": draw_queries_broad(jax.random.fold_in(streams_of[14], 71), 0),
        "keys_broad": draw_keys_broad(jax.random.fold_in(streams_of[14], 71), 0),
        "values_broad": bell_draw(streams_of[6], (CONTEXT_LENGTH, B_HEADS * B_DIM), 1.0, 6.0, ((0, 16), (1, 2))),
        "gates_narrow": draw_gates_narrow(jax.random.fold_in(streams_of[14], 71), 0),
        "gates_broad": draw_gates_broad(jax.random.fold_in(streams_of[14], 71), 0),
        "project_narrow": bell_draw(streams_of[9], (A_HEADS * A_DIM, D), ((A_HEADS * A_DIM + B_HEADS * B_DIM) // 8) ** -0.5, 0.5, ((0, 2),)),
        "project_broad": bell_draw(streams_of[10], (B_HEADS * B_DIM, D), ((A_HEADS * A_DIM + B_HEADS * B_DIM) // 8) ** -0.5, 0.5, ((0, 2),)),
        "norm_gain": jnp.clip(1.0 + 0.18 * jax.random.normal(streams_of[11], (D,), jnp.float32), 0.1, 1.9),
        "up_weight": bell_draw(streams_of[12], (D, FF), D ** -0.5, 0.125, ((0, 16), (1, 2))),
        "down_weight": bell_draw(streams_of[13], (FF, D), FF ** -0.5, 0.0625, ((0, 2), (1, 16))),
    }


def group_attention(queries, keys, values, gates, head_size):
    total_rows = queries.shape[0]
    heads = queries.shape[1] // head_size
    block = min(512, total_rows)
    blocks = total_rows // block
    query_blocks = queries.astype(jnp.float32).reshape(blocks, block, heads, head_size)
    gate_blocks = gates.reshape(blocks, block, heads)
    key_heads = keys.astype(jnp.float32).reshape(total_rows, heads, head_size)
    value_heads = values.astype(jnp.float32).reshape(total_rows, heads, head_size)
    key_pos = jnp.arange(total_rows, dtype=jnp.int32)

    def one_block(inputs):
        index, query_block, gate_block = inputs
        scores = jnp.einsum('qhd,khd->hqk', query_block, key_heads) * head_size ** (-0.5)
        scores = scores + gate_block.T[:, :, None] - gates.T[:, None, :]
        query_pos = index * block + jnp.arange(block, dtype=jnp.int32)
        allowed = key_pos[None, :] <= query_pos[:, None]
        scores = jnp.where(allowed[None], scores, -jnp.inf)
        peak = lax.optimization_barrier(jnp.max(scores, axis=-1, keepdims=True))
        weights = jnp.exp(scores - peak)
        denom = lax.optimization_barrier(jnp.sum(weights, axis=-1))
        summed = jnp.einsum('hqk,khd->hqd', weights.astype(jnp.bfloat16).astype(jnp.float32), value_heads)
        result = summed / denom[..., None]
        return result.transpose(1, 0, 2).reshape(block, heads * head_size)
    output = lax.map(one_block, (jnp.arange(blocks, dtype=jnp.int32), query_blocks, gate_blocks))
    return output.reshape(total_rows, heads * head_size).astype(jnp.bfloat16)

def reference(residual, queries_narrow, keys_narrow, values_narrow, queries_broad, keys_broad, values_broad, gates_narrow, gates_broad, project_narrow, project_broad, norm_gain, up_weight, down_weight):
    attended_narrow = group_attention(queries_narrow, keys_narrow, values_narrow, gates_narrow, A_DIM)
    attended_broad = group_attention(queries_broad, keys_broad, values_broad, gates_broad, B_DIM)
    projected = jnp.dot(attended_narrow, project_narrow, preferred_element_type=jnp.float32)
    projected = projected + jnp.dot(attended_broad, project_broad, preferred_element_type=jnp.float32)
    mixed = (residual.astype(jnp.float32) + projected).astype(jnp.bfloat16)
    mixed_wide = mixed.astype(jnp.float32)
    scale = lax.rsqrt(lax.optimization_barrier(jnp.mean(mixed_wide * mixed_wide, axis=-1, keepdims=True)) + 1e-06)
    normed = (mixed_wide * scale * norm_gain.astype(jnp.float32)).astype(jnp.bfloat16)
    hidden = jnp.square(jax.nn.relu(jnp.dot(normed, up_weight, preferred_element_type=jnp.float32))).astype(jnp.bfloat16)
    return (mixed_wide + jnp.dot(hidden, down_weight, preferred_element_type=jnp.float32)).astype(jnp.bfloat16)
```

```python
import functools

import jax
import jax.numpy as jnp
from jax import lax
from jax.experimental import pallas as pl
from jax.experimental.pallas import tpu as pltpu
from jax.sharding import PartitionSpec as P

A_DIM = 32
B_DIM = 64


def rms_scaled(mixed, norm_gain):
    mixed_wide = mixed.astype(jnp.float32)
    scale = lax.rsqrt(jnp.mean(mixed_wide * mixed_wide, axis=-1, keepdims=True) + 1e-06)
    return (mixed_wide * scale * norm_gain).astype(jnp.bfloat16)


def group_size(sp_count):
    return 8 if sp_count % 8 == 0 else sp_count


def head_columns(narrow_heads):
    ranges = [(h * A_DIM, (h + 1) * A_DIM, A_DIM) for h in range(narrow_heads)]
    return ranges + [(narrow_heads * A_DIM, narrow_heads * A_DIM + B_DIM, B_DIM)]


def attend_block(ranges, block, query, kv_all, gate_all):
    tokens, width = query.shape
    lane = lax.broadcasted_iota(jnp.int32, (tokens, width), 1)
    row = lax.broadcasted_iota(jnp.int32, (tokens, tokens), 0)
    column = lax.broadcasted_iota(jnp.int32, (tokens, tokens), 1)
    inside = [(lane >= low) & (lane < high) for low, high, _ in ranges]
    wide = query.astype(jnp.float32)
    head_queries = [jnp.where(mask, wide, 0.0).astype(jnp.bfloat16) for mask in inside]
    own_gates = gate_all[block]
    query_gates = [
        jnp.sum(jnp.where(row == column, own_gates[h : h + 1, :], 0.0), axis=1, keepdims=True)
        for h in range(len(ranges))
    ]

    def by_head(columns):
        spread = jnp.broadcast_to(columns[-1], (tokens, width))
        for mask, values in zip(inside[:-1], columns[:-1]):
            spread = jnp.where(mask, values, spread)
        return spread

    def step(key_block, state):
        peaks, totals, summed = state
        keys = kv_all[key_block, :, :width]
        values = kv_all[key_block, :, width:]
        key_gates = gate_all[key_block]
        allowed = column + (key_block - block) * tokens <= row
        new_peaks, new_totals, fades, terms = [], [], [], []
        for h, (_, _, size) in enumerate(ranges):
            scores = (
                lax.dot_general(
                    head_queries[h],
                    keys,
                    (((1,), (1,)), ((), ())),
                    preferred_element_type=jnp.float32,
                )
                * size ** (-0.5)
                + query_gates[h]
                - key_gates[h : h + 1, :]
            )
            scores = jnp.where(allowed, scores, -1e30)
            peak = jnp.maximum(peaks[h], jnp.max(scores, axis=1, keepdims=True))
            weights = jnp.exp(scores - peak)
            fade = jnp.exp(peaks[h] - peak)
            new_peaks.append(peak)
            new_totals.append(totals[h] * fade + jnp.sum(weights, axis=1, keepdims=True))
            fades.append(fade)
            terms.append(
                jnp.dot(
                    weights.astype(jnp.bfloat16), values, preferred_element_type=jnp.float32
                )
            )
        summed = summed * by_head(fades) + by_head(terms)
        return tuple(new_peaks), tuple(new_totals), summed

    heads = len(ranges)
    initial = (
        tuple(jnp.full((tokens, 1), -1e30, jnp.float32) for _ in range(heads)),
        tuple(jnp.zeros((tokens, 1), jnp.float32) for _ in range(heads)),
        jnp.zeros((tokens, width), jnp.float32),
    )
    _, totals, summed = lax.fori_loop(0, block + 1, step, initial)
    return (summed / by_head(totals)).astype(jnp.bfloat16)


def layer_kernel(
    count,
    group,
    ranges,
    q_ref,
    kv_ref,
    gate_ref,
    up_ref,
    down_ref,
    attended_out,
    up_out,
    down_out,
    q_all,
    kv_all,
    gate_all,
    attended,
    up_hold,
    down_hold,
    kv_sems,
    gate_sems,
    q_sems,
    back_sems,
    sems,
    own_sems,
):
    me = lax.axis_index("sp")
    head_groups = q_ref.shape[0]
    parts = count // head_groups
    my_heads = me % head_groups
    my_part = me // head_groups

    def block_of(part, slot):
        turn = slot % 2
        return slot * parts + (1 - turn) * part + turn * (parts - 1 - part)

    my_slot = me // parts
    my_turn = my_slot % 2
    place = me % parts
    reader_part = (1 - my_turn) * place + my_turn * (parts - 1 - place)
    up_rows = up_ref.shape[0]
    units = up_out.shape[1]
    columns = down_ref.shape[1]
    barrier = pltpu.get_barrier_semaphore()

    def hello(k, carry):
        pl.semaphore_signal(
            barrier,
            inc=1,
            device_id={"sp": (me + k) % count},
            device_id_type=pl.DeviceIdType.MESH,
        )
        return carry

    lax.fori_loop(1, count, hello, 0)
    pl.semaphore_wait(barrier, count - 1)

    def remote(source, target, sem_pair, first, second, peer):
        return pltpu.make_async_remote_copy(
            src_ref=source,
            dst_ref=target,
            send_sem=sem_pair.at[0, first],
            recv_sem=sem_pair.at[1, second],
            device_id={"sp": peer},
            device_id_type=pl.DeviceIdType.MESH,
        )

    def context_copies(k, owner):
        peer = (me + k) % count
        heads = peer % head_groups
        return (
            remote(kv_ref.at[heads], kv_all.at[owner], kv_sems, k, k, peer),
            remote(gate_ref.at[heads], gate_all.at[owner], gate_sems, k, k, peer),
        )

    def start_context(k, carry):
        for copy in context_copies(k, me):
            copy.start()
        return carry

    def wait_context(k, carry):
        for copy in context_copies(k, (me + count - k) % count):
            copy.wait_recv()
            copy.wait_send()
        return carry

    for heads in range(head_groups):
        reader = reader_part * head_groups + heads

        @pl.when(reader != me)
        def _():
            remote(q_ref.at[heads], q_all.at[my_slot], q_sems, heads, my_slot, reader).start()

        @pl.when(reader == me)
        def _():
            q_all[my_slot] = q_ref[heads]

    lax.fori_loop(1, count, start_context, 0)
    kv_all[me] = kv_ref[my_heads]
    gate_all[me] = gate_ref[my_heads]

    def up_source(chunk):
        return up_ref.at[:, pl.ds(pl.multiple_of(chunk * units, 128), units)]

    def down_source(chunk):
        return down_ref.at[pl.ds(pl.multiple_of(chunk * units, units), units), :]

    def up_target(owner):
        return up_out.at[pl.ds(pl.multiple_of(owner * up_rows, up_rows), up_rows), :]

    def down_target(owner):
        if len(down_out.shape) == 3:
            return down_out.at[owner]
        return down_out.at[:, pl.ds(pl.multiple_of(owner * columns, columns), columns)]

    def copies(k, target_owner):
        peer = (me + k) % count
        chunk = peer % group
        pairs = (
            (up_source(chunk), up_target(target_owner)),
            (down_source(chunk), down_target(target_owner)),
        )
        return [
            pltpu.make_async_remote_copy(
                src_ref=source,
                dst_ref=target,
                send_sem=sems.at[0, which, k],
                recv_sem=sems.at[1, which, k],
                device_id={"sp": peer},
                device_id_type=pl.DeviceIdType.MESH,
            )
            for which, (source, target) in enumerate(pairs)
        ]

    def start(k, carry):
        for copy in copies(k, me):
            copy.start()
        return carry

    def finish(k, carry):
        for copy in copies(k, (me + count - k) % count):
            copy.wait_recv()
            copy.wait_send()
        return carry

    lax.fori_loop(1, count, start, 0)
    own = me % group
    first = [
        pltpu.make_async_copy(up_source(own), up_hold, own_sems.at[0]),
        pltpu.make_async_copy(down_source(own), down_hold, own_sems.at[1]),
    ]
    for copy in first:
        copy.start()
    for copy in first:
        copy.wait()
    second = [
        pltpu.make_async_copy(up_hold, up_target(me), own_sems.at[0]),
        pltpu.make_async_copy(down_hold, down_target(me), own_sems.at[1]),
    ]
    for copy in second:
        copy.start()
    for heads in range(head_groups):
        reader = reader_part * head_groups + heads

        @pl.when(reader != me)
        def _():
            remote(q_ref.at[heads], q_all.at[my_slot], q_sems, heads, my_slot, reader).wait_send()

    for slot in range(head_groups):
        owner = block_of(my_part, slot)

        @pl.when(owner != me)
        def _():
            remote(q_ref.at[0], q_all.at[slot], q_sems, 0, slot, owner).wait_recv()

    lax.fori_loop(1, count, wait_context, 0)

    def attend(slot, carry):
        block = block_of(my_part, slot)
        attended[slot] = attend_block(ranges, block, q_all[slot], kv_all, gate_all)
        return carry

    lax.fori_loop(0, head_groups, attend, 0)
    for slot in range(head_groups):
        owner = block_of(my_part, slot)

        @pl.when(owner != me)
        def _():
            remote(
                attended.at[slot], attended_out.at[my_heads], back_sems, slot, my_heads, owner
            ).start()

        @pl.when(owner == me)
        def _():
            attended_out[my_heads] = attended[slot]

    for copy in second:
        copy.wait()
    lax.fori_loop(1, count, finish, 0)
    for slot in range(head_groups):
        owner = block_of(my_part, slot)

        @pl.when(owner != me)
        def _():
            remote(
                attended.at[slot], attended_out.at[my_heads], back_sems, slot, my_heads, owner
            ).wait_send()

    for heads in range(head_groups):
        reader = reader_part * head_groups + heads

        @pl.when(reader != me)
        def _():
            remote(
                attended.at[0], attended_out.at[heads], back_sems, 0, heads, reader
            ).wait_recv()


def attend_and_share(queries, keys_values, gates, ranges, up_weight, down_weight):
    head_groups, tokens, head_width = queries.shape
    count = lax.axis_size("sp")
    group = group_size(count)
    up_rows, unit_total = up_weight.shape
    columns = down_weight.shape[1]
    units = unit_total // group
    if columns % 128 == 0:
        down_shape = (units, count * columns)
    else:
        down_shape = (count, units, columns)
    attended, up_full, down_full = pl.pallas_call(
        functools.partial(layer_kernel, count, group, ranges),
        out_shape=(
            jax.ShapeDtypeStruct(queries.shape, queries.dtype),
            jax.ShapeDtypeStruct((count * up_rows, units), up_weight.dtype),
            jax.ShapeDtypeStruct(down_shape, down_weight.dtype),
        ),
        in_specs=[pl.BlockSpec(memory_space=pltpu.VMEM)] * 3
        + [pl.BlockSpec(memory_space=pl.ANY)] * 2,
        out_specs=[pl.BlockSpec(memory_space=pltpu.VMEM)]
        + [pl.BlockSpec(memory_space=pl.ANY)] * 2,
        scratch_shapes=[
            pltpu.VMEM(queries.shape, queries.dtype),
            pltpu.VMEM((count,) + keys_values.shape[1:], keys_values.dtype),
            pltpu.VMEM((count,) + gates.shape[1:], gates.dtype),
            pltpu.VMEM(queries.shape, queries.dtype),
            pltpu.VMEM((up_rows, units), up_weight.dtype),
            pltpu.VMEM((units, columns), down_weight.dtype),
            pltpu.SemaphoreType.DMA((2, count)),
            pltpu.SemaphoreType.DMA((2, count)),
            pltpu.SemaphoreType.DMA((2, head_groups)),
            pltpu.SemaphoreType.DMA((2, head_groups)),
            pltpu.SemaphoreType.DMA((2, 2, count)),
            pltpu.SemaphoreType.DMA((2,)),
        ],
        compiler_params=pltpu.CompilerParams(collective_id=0, has_side_effects=True),
        cost_estimate=pl.CostEstimate(
            flops=0, bytes_accessed=count * up_rows * units * 80, transcendentals=0
        ),
    )(queries, keys_values, gates, up_weight, down_weight)
    if columns % 128:
        down_full = down_full.transpose(1, 0, 2).reshape(units, count * columns)
    return attended, up_full, down_full


def gather_kernel(group, tp_count, rows_ref, out_ref, hold, sems, own_sems, pass_sems):
    sp = lax.axis_index("sp")
    tp = lax.axis_index("tp")
    base = (sp // group) * group
    me = sp - base
    barrier = pltpu.get_barrier_semaphore()
    for k in range(1, group):
        pl.semaphore_signal(
            barrier,
            inc=1,
            device_id={"sp": base + (me + k) % group},
            device_id_type=pl.DeviceIdType.MESH,
        )
    for j in range(1, tp_count):
        pl.semaphore_signal(
            barrier,
            inc=1,
            device_id={"tp": (tp + j) % tp_count},
            device_id_type=pl.DeviceIdType.MESH,
        )
    pl.semaphore_wait(barrier, group + tp_count - 2)

    def across(k, owner):
        return pltpu.make_async_remote_copy(
            src_ref=rows_ref,
            dst_ref=out_ref.at[tp, owner],
            send_sem=sems.at[0, k],
            recv_sem=sems.at[1, k],
            device_id={"sp": base + (me + k) % group},
            device_id_type=pl.DeviceIdType.MESH,
        )

    def beside(j, k, source, tp_owner, owner):
        return pltpu.make_async_remote_copy(
            src_ref=source,
            dst_ref=out_ref.at[tp_owner, owner],
            send_sem=pass_sems.at[0, j, k],
            recv_sem=pass_sems.at[1, j, k],
            device_id={"tp": (tp + j) % tp_count},
            device_id_type=pl.DeviceIdType.MESH,
        )

    for k in range(1, group):
        across(k, me).start()
    for j in range(1, tp_count):
        beside(j, 0, rows_ref, tp, me).start()
    own = pltpu.make_async_copy(rows_ref, hold, own_sems.at[0])
    own.start()
    own.wait()
    own = pltpu.make_async_copy(hold, out_ref.at[tp, me], own_sems.at[1])
    own.start()
    own.wait()
    for k in range(1, group):
        owner = (me + group - k) % group
        across(k, owner).wait_recv()
        for j in range(1, tp_count):
            beside(j, k, out_ref.at[tp, owner], tp, owner).start()
    for k in range(1, group):
        across(k, me).wait_send()
    for j in range(1, tp_count):
        for k in range(group):
            owner = (me + group - k) % group
            copy = beside(j, k, rows_ref, (tp + tp_count - j) % tp_count, owner)
            copy.wait_send()
            copy.wait_recv()


def gather_rows(rows):
    group = group_size(lax.axis_size("sp"))
    tp_count = lax.axis_size("tp")
    return pl.pallas_call(
        functools.partial(gather_kernel, group, tp_count),
        out_shape=jax.ShapeDtypeStruct((tp_count, group) + rows.shape, rows.dtype),
        in_specs=[pl.BlockSpec(memory_space=pl.ANY)],
        out_specs=pl.BlockSpec(memory_space=pl.ANY),
        scratch_shapes=[
            pltpu.VMEM(rows.shape, rows.dtype),
            pltpu.SemaphoreType.DMA((2, group)),
            pltpu.SemaphoreType.DMA((2,)),
            pltpu.SemaphoreType.DMA((2, tp_count, group)),
        ],
        compiler_params=pltpu.CompilerParams(collective_id=1, has_side_effects=True),
    )(rows)


def return_kernel(group, parts_ref, out_ref, hold, sems, own_sems):
    sp = lax.axis_index("sp")
    base = (sp // group) * group
    me = sp - base
    barrier = pltpu.get_barrier_semaphore()
    for k in range(1, group):
        pl.semaphore_signal(
            barrier,
            inc=1,
            device_id={"sp": base + (me + k) % group},
            device_id_type=pl.DeviceIdType.MESH,
        )
    pl.semaphore_wait(barrier, group - 1)

    def across(k, owner):
        peer = (me + k) % group
        return pltpu.make_async_remote_copy(
            src_ref=parts_ref.at[peer],
            dst_ref=out_ref.at[owner],
            send_sem=sems.at[0, k],
            recv_sem=sems.at[1, k],
            device_id={"sp": base + peer},
            device_id_type=pl.DeviceIdType.MESH,
        )

    for k in range(1, group):
        across(k, me).start()
    own = pltpu.make_async_copy(parts_ref.at[me], hold, own_sems.at[0])
    own.start()
    own.wait()
    own = pltpu.make_async_copy(hold, out_ref.at[me], own_sems.at[1])
    own.start()
    own.wait()
    for k in range(1, group):
        copy = across(k, (me + group - k) % group)
        copy.wait_recv()
        copy.wait_send()


def return_parts(parts):
    group = parts.shape[0]
    return pl.pallas_call(
        functools.partial(return_kernel, group),
        out_shape=jax.ShapeDtypeStruct(parts.shape, parts.dtype),
        in_specs=[pl.BlockSpec(memory_space=pl.ANY)],
        out_specs=pl.BlockSpec(memory_space=pl.ANY),
        scratch_shapes=[
            pltpu.VMEM(parts.shape[1:], parts.dtype),
            pltpu.SemaphoreType.DMA((2, group)),
            pltpu.SemaphoreType.DMA((2,)),
        ],
        compiler_params=pltpu.CompilerParams(collective_id=2, has_side_effects=True),
    )(parts)


def local(
    residual,
    queries_narrow,
    keys_narrow,
    values_narrow,
    queries_broad,
    keys_broad,
    values_broad,
    gates_narrow,
    gates_broad,
    project_narrow,
    project_broad,
    norm_gain,
    up_weight,
    down_weight,
):
    tokens = queries_narrow.shape[0]
    head_groups = gates_broad.shape[1]
    narrow_heads = gates_narrow.shape[1] // head_groups
    ranges = head_columns(narrow_heads)

    def by_group(narrow, broad):
        return jnp.concatenate(
            [part.reshape(tokens, head_groups, -1) for part in (narrow, broad)], axis=-1
        ).transpose(1, 0, 2)

    gates = jnp.concatenate(
        [gates_narrow.reshape(tokens, head_groups, narrow_heads), gates_broad[..., None]], axis=-1
    ).transpose(1, 2, 0)
    gates = jnp.pad(gates, ((0, 0), (0, -gates.shape[1] % 8), (0, 0)))
    attended, up_full, down_full = attend_and_share(
        by_group(queries_narrow, queries_broad),
        jnp.concatenate(
            [by_group(keys_narrow, keys_broad), by_group(values_narrow, values_broad)], axis=-1
        ),
        gates,
        ranges,
        up_weight,
        down_weight,
    )
    rows_first = attended.transpose(1, 0, 2)
    split = narrow_heads * A_DIM
    attended_narrow = rows_first[..., :split].reshape(tokens, -1)
    attended_broad = rows_first[..., split:].reshape(tokens, -1)
    projected = lax.psum_scatter(
        (
            jnp.dot(attended_narrow, project_narrow, preferred_element_type=jnp.float32)
            + jnp.dot(attended_broad, project_broad, preferred_element_type=jnp.float32)
        ).astype(jnp.bfloat16),
        "tp",
        scatter_dimension=0,
        tiled=True,
    ).astype(jnp.float32)
    mixed = (residual.astype(jnp.float32) + projected).astype(jnp.bfloat16)
    features = gather_rows(rms_scaled(mixed, norm_gain))
    tp_count, group, rows, width = features.shape
    up_total = jnp.dot(
        features.reshape(tp_count * group * rows, width),
        up_full,
        preferred_element_type=jnp.float32,
    )
    hidden = jnp.square(jax.nn.relu(up_total)).astype(jnp.bfloat16)
    down_term = jnp.dot(hidden, down_full, preferred_element_type=jnp.float32)
    parts = lax.psum_scatter(
        down_term.astype(jnp.bfloat16).reshape(features.shape),
        "tp",
        scatter_dimension=0,
        tiled=False,
    )
    summed_rows = jnp.sum(return_parts(parts).astype(jnp.float32), axis=0)
    return (mixed.astype(jnp.float32) + summed_rows).astype(jnp.bfloat16)


LOG2E = 1.4426950408889634
PIECES = 3
GATE_ROWS = 16


def split_pieces(values):
    pieces = []
    rest = values
    for _ in range(PIECES):
        piece = rest.astype(jnp.bfloat16).astype(jnp.float32)
        pieces.append(piece)
        rest = rest - piece
    return pieces


def pad_rows(values, rows):
    return jnp.concatenate(
        [values, jnp.zeros((rows - values.shape[0], values.shape[1]), values.dtype)], axis=0
    )


def pad_lanes(values, lanes):
    return jnp.concatenate(
        [values, jnp.zeros((values.shape[0], lanes - values.shape[1]), values.dtype)], axis=1
    )


def fused_kernel(
    count,
    group,
    head_groups,
    ranges,
    residual_ref,
    qn_ref,
    kn_ref,
    vn_ref,
    qb_ref,
    kb_ref,
    vb_ref,
    gn_ref,
    gb_ref,
    gain_ref,
    pn_ref,
    pb_ref,
    up_ref,
    down_ref,
    out_ref,
    q_send,
    kv_send,
    gate_send,
    q_all,
    kv_all,
    gate_all,
    key_gates,
    v_turned,
    q_wide,
    acc,
    attended,
    attended_in,
    project,
    mixed,
    normed,
    up_all,
    down_all,
    features,
    hidden,
    part_out,
    part_in,
    return_out,
    return_in,
    kv_line,
    gate_line,
    kv_plane,
    gate_plane,
    q_sems,
    back_sems,
    project_own,
    project_sems,
    weight_sems,
    own_sems,
    across_sems,
    beside_sems,
    part_sems,
    return_sems,
):
    me = lax.axis_index("sp")
    tp = lax.axis_index("tp")
    other = 1 - tp
    planes = head_groups
    parts = count // planes
    plane = me // parts
    lane = me % parts
    base = (me // group) * group
    local = me - base
    tokens, _ = qn_ref.shape
    rows, width = residual_ref.shape
    heads = len(ranges)
    head_width = q_send.shape[2]
    narrow_width = ranges[-1][0]
    broad_width = head_width - narrow_width
    span = 2 * tokens
    barrier = pltpu.get_barrier_semaphore()

    def remote(source, target, send, recv, sp, core):
        return pltpu.make_async_remote_copy(
            src_ref=source,
            dst_ref=target,
            send_sem=send,
            recv_sem=recv,
            device_id={"sp": sp, "tp": core},
            device_id_type=pl.DeviceIdType.MESH,
        )

    def hello(k, carry):
        flat = (me * 2 + tp + k) % (count * 2)
        pl.semaphore_signal(
            barrier,
            inc=1,
            device_id={"sp": flat // 2, "tp": flat % 2},
            device_id_type=pl.DeviceIdType.MESH,
        )
        return carry

    lax.fori_loop(1, count * 2, hello, 0)

    def by_group(narrow_ref, broad_ref, h):
        return [
            narrow_ref[:, h * narrow_width : (h + 1) * narrow_width],
            broad_ref[:, h * broad_width : (h + 1) * broad_width],
        ]

    narrow_heads = heads - 1
    gates = pad_lanes(jnp.concatenate([gn_ref[...], gb_ref[...]], axis=1), 128)
    gates = pad_rows(gates, -(-tokens // 128) * 128).T[:, :tokens]
    for h in range(head_groups):
        kv_send[h] = jnp.concatenate(
            by_group(kn_ref, kb_ref, h) + by_group(vn_ref, vb_ref, h), axis=1
        )
        q_send[h] = jnp.concatenate(by_group(qn_ref, qb_ref, h), axis=1)
        lines = []
        for i, (_, _, size) in enumerate(ranges):
            if i < narrow_heads:
                source = h * narrow_heads + i
            else:
                source = head_groups * narrow_heads + h
            lines += split_pieces(gates[source : source + 1] * size**0.5)
        lines += [jnp.ones((PIECES, tokens), jnp.float32)]
        gate_send[h] = pad_rows(jnp.concatenate(lines, axis=0), GATE_ROWS).astype(jnp.bfloat16)

    pl.semaphore_wait(barrier, count * 2 - 1)

    def line_copies(j, owner):
        target = (plane + j) % planes
        peer = target * parts + lane
        return (
            remote(
                kv_send.at[target], kv_all.at[owner], kv_line.at[0, j], kv_line.at[1, j], peer, tp
            ),
            remote(
                gate_send.at[target],
                gate_all.at[owner],
                gate_line.at[0, j],
                gate_line.at[1, j],
                peer,
                tp,
            ),
        )

    def line_owner(j):
        return ((plane + planes - j) % planes) * parts + lane

    def plane_copies(j, k, kv_source, gate_source, owner):
        peer = plane * parts + (lane + k) % parts
        return (
            remote(
                kv_source,
                kv_all.at[owner],
                kv_plane.at[0, j, k],
                kv_plane.at[1, j, k],
                peer,
                tp,
            ),
            remote(
                gate_source,
                gate_all.at[owner],
                gate_plane.at[0, j, k],
                gate_plane.at[1, j, k],
                peer,
                tp,
            ),
        )

    for j in range(1, planes):
        for copy in line_copies(j, me):
            copy.start()
    for k in range(1, parts):
        for copy in plane_copies(0, k, kv_send.at[plane], gate_send.at[plane], me):
            copy.start()
    kv_all[me] = kv_send[plane]
    gate_all[me] = gate_send[plane]

    double = me // 2
    reader_part = jnp.where(double < parts, double, 2 * parts - 1 - double)
    my_slot = 2 * (double // parts) + me % 2

    def tile_double(tile):
        return tile * (2 * parts - 1 - lane) + (1 - tile) * lane

    for h in range(head_groups):
        reader = h * parts + reader_part

        @pl.when(reader != me)
        def _():
            remote(
                q_send.at[h], q_all.at[my_slot], q_sems.at[0, h], q_sems.at[1, my_slot], reader, tp
            ).start()

        @pl.when(reader == me)
        def _():
            q_all[my_slot] = q_send[h]

    def project_pairs(h):
        pairs = []
        for source, low, size in (
            (pn_ref, 0, narrow_width),
            (pb_ref, narrow_width, broad_width),
        ):
            pairs.append(
                (
                    source.at[h * size : (h + 1) * size, :],
                    project.at[tp * head_groups + h, low : low + size, :],
                )
            )
        return pairs

    def project_copies(h):
        own, away = [], []
        for i, (source, target) in enumerate(project_pairs(h)):
            own.append(pltpu.make_async_copy(source, target, project_own.at[h, i]))
            away.append(
                remote(
                    source,
                    target,
                    project_sems.at[0, h, i],
                    project_sems.at[1, h, i],
                    me,
                    other,
                )
            )
        return own, away

    for h in range(head_groups):
        own, away = project_copies(h)
        for copy in own + away:
            copy.start()

    units = up_all.shape[2]

    def up_source(chunk):
        return up_ref.at[:, pl.ds(pl.multiple_of(chunk * units, 128), units)]

    def down_source(chunk):
        return down_ref.at[pl.ds(pl.multiple_of(chunk * units, units), units), :]

    def weight_copy(which, k, owner):
        peer = (me + k) % count
        chunk = peer % group
        source = up_source(chunk) if which == 0 else down_source(chunk)
        target = up_all.at[owner] if which == 0 else down_all.at[owner]
        return remote(
            source, target, weight_sems.at[0, which, k], weight_sems.at[1, which, k], peer, tp
        )

    own_weights = [
        pltpu.make_async_copy(up_source(local), up_all.at[me], own_sems.at[0]),
        pltpu.make_async_copy(down_source(local), down_all.at[me], own_sems.at[1]),
    ]
    for copy in own_weights:
        copy.start()

    for j in range(1, planes):
        owner = line_owner(j)
        for copy in line_copies(j, owner):
            copy.wait_recv()
        for k in range(1, parts):
            for copy in plane_copies(j, k, kv_all.at[owner], gate_all.at[owner], owner):
                copy.start()

    def start_weights(which):
        def start(k, carry):
            weight_copy(which, k, me).start()
            return carry

        lax.fori_loop(1, count, start, 0)

    start_weights(0)
    start_weights(1)

    for j in range(planes):
        for k in range(1, parts):
            owner = ((plane + planes - j) % planes) * parts + (lane + parts - k) % parts
            for copy in plane_copies(j, k, kv_all.at[owner], gate_all.at[owner], owner):
                copy.wait_recv()

    def turn(pair, carry):
        values = kv_all[pl.ds(2 * pair, 2), :, head_width:].reshape(span, head_width)
        v_turned[pair] = values.astype(jnp.float32).T.astype(jnp.bfloat16)
        for i in range(2):
            block = pad_rows(gate_all[2 * pair + i].astype(jnp.float32), 128)
            block = pad_lanes(block, -(-tokens // 128) * 128).T[:tokens]
            key_gates[2 * pair + i] = block.astype(jnp.bfloat16)
        return carry

    lax.fori_loop(0, count // 2, turn, 0)

    for slot in range(4):
        owner = 2 * tile_double(slot // 2) + slot % 2

        @pl.when(owner != me)
        def _():
            remote(
                q_send.at[0], q_all.at[slot], q_sems.at[0, 0], q_sems.at[1, slot], owner, tp
            ).wait_recv()

    lane_id = lax.broadcasted_iota(jnp.int32, (span, head_width), 1)
    first_one = heads * PIECES

    def attend(tile, carry):
        double_block = tile_double(tile)
        query = q_all[pl.ds(2 * tile, 2)].reshape(span, head_width).astype(jnp.float32)
        own_gates = (
            key_gates[pl.ds(2 * double_block, 2)].reshape(span, head_width).astype(jnp.float32)
        )
        for i, (low, high, _) in enumerate(ranges):
            left = jnp.where((lane_id >= low) & (lane_id < high), query, 0.0)
            moved = pltpu.roll(own_gates, first_one - i * PIECES, 1)
            right = jnp.where((lane_id >= first_one) & (lane_id < first_one + PIECES), moved, 0.0)
            right = jnp.where(
                (lane_id >= i * PIECES) & (lane_id < (i + 1) * PIECES), -1.0, right
            )
            q_wide[i] = jnp.concatenate([left, right], axis=1).astype(jnp.bfloat16)
        acc[...] = jnp.zeros_like(acc)

        def step(pair, state, masked):
            peaks, totals = state
            keys = jnp.concatenate(
                [
                    kv_all[pl.ds(2 * pair, 2), :, :head_width].reshape(span, head_width),
                    key_gates[pl.ds(2 * pair, 2)].reshape(span, head_width),
                ],
                axis=1,
            )
            new_peaks, new_totals = [], []
            for i, (low, high, size) in enumerate(ranges):
                factor = size**-0.5 * LOG2E
                scores = lax.dot_general(
                    keys, q_wide[i], (((1,), (1,)), ((), ())), preferred_element_type=jnp.float32
                )
                if masked:
                    row = lax.broadcasted_iota(jnp.int32, (span, span), 0)
                    column = lax.broadcasted_iota(jnp.int32, (span, span), 1)
                    scores = jnp.where(row <= column, scores, -1e30)
                peak = jnp.maximum(peaks[i], jnp.max(scores, axis=0, keepdims=True))
                weights = jnp.exp2((scores - peak) * factor)
                fade = jnp.exp2((peaks[i] - peak) * factor)
                new_peaks.append(peak)
                new_totals.append(totals[i] * fade + jnp.sum(weights, axis=0, keepdims=True))
                acc[low:high, :] = acc[low:high, :] * fade + jnp.dot(
                    v_turned[pair, low:high, :],
                    weights.astype(jnp.bfloat16),
                    preferred_element_type=jnp.float32,
                )
            return tuple(new_peaks), tuple(new_totals)

        state = (
            tuple(jnp.full((1, span), -1e30, jnp.float32) for _ in ranges),
            tuple(jnp.zeros((1, span), jnp.float32) for _ in ranges),
        )
        state = lax.fori_loop(
            0, double_block, lambda pair, state: step(pair, state, False), state
        )
        _, totals = step(double_block, state, True)
        scaled = jnp.concatenate(
            [acc[low:high, :] / totals[i] for i, (low, high, _) in enumerate(ranges)], axis=0
        )
        attended[pl.ds(2 * tile, 2)] = (
            scaled.T.astype(jnp.bfloat16).reshape(2, tokens, head_width)
        )
        return carry

    lax.fori_loop(0, 2, attend, 0)

    def back_copy(slot, core, place, sp):
        return remote(
            attended.at[slot, core * rows : (core + 1) * rows, :],
            attended_in.at[place],
            back_sems.at[0, slot, core],
            back_sems.at[1, 0, place],
            sp,
            core,
        )

    my_place = tp * head_groups + plane
    for slot in range(4):
        owner = 2 * tile_double(slot // 2) + slot % 2
        for core in range(2):
            here = (owner == me) & (tp == core)

            @pl.when(jnp.logical_not(here))
            def _():
                back_copy(slot, core, my_place, owner).start()

            @pl.when(here)
            def _():
                attended_in[my_place] = attended[slot, core * rows : (core + 1) * rows, :]

    for h in range(head_groups):
        own, away = project_copies(h)
        for copy in own:
            copy.wait()
        for copy in away:
            copy.wait()
    for h in range(head_groups):
        for core in range(2):
            place = core * head_groups + h
            sender = h * parts + reader_part

            @pl.when(jnp.logical_not((sender == me) & (tp == core)))
            def _():
                remote(
                    attended.at[0, :rows, :],
                    attended_in.at[place],
                    back_sems.at[0, 0, 0],
                    back_sems.at[1, 0, place],
                    sender,
                    core,
                ).wait_recv()

    step_width = return_out.shape[3]
    chunks = width // step_width
    joined = jnp.concatenate([attended_in[i] for i in range(2 * head_groups)], axis=1)

    def project_step(n, squares):
        columns = pl.ds(pl.multiple_of(n * step_width, step_width), step_width)
        total = residual_ref[:, columns].astype(jnp.float32) + jnp.dot(
            joined,
            project[:, :, columns].reshape(2 * head_groups * head_width, step_width),
            preferred_element_type=jnp.float32,
        )
        total = total.astype(jnp.bfloat16).astype(jnp.float32)
        mixed[:, columns] = total
        return squares + jnp.sum(total * total, axis=1, keepdims=True)

    squares = lax.fori_loop(0, chunks, project_step, jnp.zeros((rows, 1), jnp.float32))
    scale = lax.rsqrt(squares / width + 1e-06)
    scaled_rows = (mixed[...] * scale * gain_ref[...]).astype(jnp.bfloat16)
    normed[...] = scaled_rows
    features[tp, local] = scaled_rows

    def across(k, owner):
        return remote(
            normed,
            features.at[tp, owner],
            across_sems.at[0, k],
            across_sems.at[1, k],
            base + (local + k) % group,
            tp,
        )

    def beside(k, source, core, owner):
        return remote(
            source,
            features.at[core, owner],
            beside_sems.at[0, k],
            beside_sems.at[1, k],
            me,
            other,
        )

    for k in range(1, group):
        across(k, local).start()
    beside(0, normed, tp, local).start()

    def pass_on(k, carry):
        owner = (local + group - k) % group
        across(k, owner).wait_recv()
        beside(k, features.at[tp, owner], tp, owner).start()
        return carry

    lax.fori_loop(1, group, pass_on, 0)

    def receive_pass(k, carry):
        owner = (local + group - k) % group
        beside(k, normed, other, owner).wait_recv()
        return carry

    lax.fori_loop(0, group, receive_pass, 0)

    def wait_weights(which, k):
        copy = weight_copy(which, k, (me + count - k) % count)
        copy.wait_recv()

    own_weights[0].wait()

    def wait_up(k, carry):
        wait_weights(0, k)
        return carry

    lax.fori_loop(1, count, wait_up, 0)
    row_groups = 2
    some = group // row_groups

    def up_step(i, carry):
        core = (other + i // row_groups) % 2
        chips = pl.ds((i % row_groups) * some, some)
        total = jnp.dot(
            features[core, chips].reshape(some * rows, width),
            up_all[...].reshape(width, units),
            preferred_element_type=jnp.float32,
        )
        total = jnp.maximum(total, 0.0)
        hidden[core, chips] = (
            (total * total).astype(jnp.bfloat16).reshape(some, rows, units)
        )
        return carry

    lax.fori_loop(0, 2 * row_groups, up_step, 0)
    own_weights[1].wait()

    def wait_down(k, carry):
        wait_weights(1, k)
        return carry

    lax.fori_loop(1, count, wait_down, 0)
    per_chunk = count // chunks

    def down_columns(chunk):
        return jnp.concatenate(
            [down_all[chunk * per_chunk + i] for i in range(per_chunk)], axis=1
        )

    def part_copy(chunk):
        return remote(
            part_out.at[chunk],
            part_in.at[chunk],
            part_sems.at[0, chunk],
            part_sems.at[1, chunk],
            me,
            other,
        )

    def down_dot(core, chips, chunk):
        return jnp.dot(
            hidden[core, chips].reshape(some * rows, units),
            down_columns(chunk),
            preferred_element_type=jnp.float32,
        ).reshape(some, rows, step_width)

    def away_step(chunk, carry):
        def inner(i, carry):
            chips = pl.ds(i * some, some)
            part_out[chunk, chips] = down_dot(other, chips, chunk).astype(jnp.bfloat16)
            return carry

        lax.fori_loop(0, row_groups, inner, 0)
        part_copy(chunk).start()
        return carry

    lax.fori_loop(0, chunks, away_step, 0)

    def return_copy(chunk, k, owner):
        peer = (local + k) % group
        return remote(
            return_out.at[chunk, peer],
            return_in.at[chunk, owner],
            return_sems.at[0, chunk, k],
            return_sems.at[1, chunk, k],
            base + peer,
            tp,
        )

    def home_step(chunk, carry):
        part_copy(chunk).wait_recv()

        def inner(i, carry):
            chips = pl.ds(i * some, some)
            return_out[chunk, chips] = (
                down_dot(tp, chips, chunk) + part_in[chunk, chips].astype(jnp.float32)
            ).astype(jnp.bfloat16)
            return carry

        lax.fori_loop(0, row_groups, inner, 0)
        for k in range(1, group):
            return_copy(chunk, k, local).start()
        return carry

    lax.fori_loop(0, chunks, home_step, 0)

    def final_step(chunk, carry):
        columns = pl.ds(pl.multiple_of(chunk * step_width, step_width), step_width)
        total = mixed[:, columns] + return_out[chunk, local].astype(jnp.float32)
        for k in range(1, group):
            owner = (local + group - k) % group
            return_copy(chunk, k, owner).wait_recv()
            total = total + return_in[chunk, owner].astype(jnp.float32)
        out_ref[:, columns] = total.astype(jnp.bfloat16)
        return carry

    lax.fori_loop(0, chunks, final_step, 0)

    for j in range(1, planes):
        for copy in line_copies(j, me):
            copy.wait_send()
    for j in range(planes):
        for k in range(1, parts):
            for copy in plane_copies(j, k, kv_send.at[plane], gate_send.at[plane], me):
                copy.wait_send()
    for h in range(head_groups):
        reader = h * parts + reader_part

        @pl.when(reader != me)
        def _():
            remote(
                q_send.at[h], q_all.at[my_slot], q_sems.at[0, h], q_sems.at[1, my_slot], reader, tp
            ).wait_send()

    for slot in range(4):
        owner = 2 * tile_double(slot // 2) + slot % 2
        for core in range(2):
            here = (owner == me) & (tp == core)

            @pl.when(jnp.logical_not(here))
            def _():
                back_copy(slot, core, my_place, owner).wait_send()

    def weights_sent(k, carry):
        for which in range(2):
            weight_copy(which, k, me).wait_send()
        return carry

    lax.fori_loop(1, count, weights_sent, 0)
    for k in range(1, group):
        across(k, local).wait_send()
    for k in range(group):
        beside(k, normed, tp, local).wait_send()

    def returns_sent(chunk, carry):
        part_copy(chunk).wait_send()
        for k in range(1, group):
            return_copy(chunk, k, local).wait_send()
        return carry

    lax.fori_loop(0, chunks, returns_sent, 0)


def fused_local(
    residual,
    queries_narrow,
    keys_narrow,
    values_narrow,
    queries_broad,
    keys_broad,
    values_broad,
    gates_narrow,
    gates_broad,
    project_narrow,
    project_broad,
    norm_gain,
    up_weight,
    down_weight,
):
    count = lax.axis_size("sp")
    group = group_size(count)
    tokens = queries_narrow.shape[0]
    rows, width = residual.shape
    head_groups = gates_broad.shape[1]
    parts = count // head_groups
    narrow_heads = gates_narrow.shape[1] // head_groups
    ranges = head_columns(narrow_heads)
    heads = len(ranges)
    head_width = ranges[-1][1]
    up_rows, unit_total = up_weight.shape
    units = unit_total // group
    columns = down_weight.shape[1]
    step_width = 4 * columns
    chunks = width // step_width
    span = 2 * tokens
    kind = residual.dtype
    vmem = pl.BlockSpec(memory_space=pltpu.VMEM)
    anywhere = pl.BlockSpec(memory_space=pl.ANY)
    dma = pltpu.SemaphoreType.DMA
    returned = (chunks, group, rows, step_width)
    return pl.pallas_call(
        functools.partial(fused_kernel, count, group, head_groups, ranges),
        out_shape=jax.ShapeDtypeStruct(residual.shape, kind),
        in_specs=[vmem] * 10 + [anywhere] * 4,
        out_specs=vmem,
        scratch_shapes=[
            pltpu.VMEM((head_groups, tokens, head_width), kind),
            pltpu.VMEM((head_groups, tokens, 2 * head_width), kind),
            pltpu.VMEM((head_groups, GATE_ROWS, tokens), kind),
            pltpu.VMEM((4, tokens, head_width), kind),
            pltpu.VMEM((count, tokens, 2 * head_width), kind),
            pltpu.VMEM((count, GATE_ROWS, tokens), kind),
            pltpu.VMEM((count, tokens, head_width), kind),
            pltpu.VMEM((count // 2, head_width, span), kind),
            pltpu.VMEM((heads, span, 2 * head_width), kind),
            pltpu.VMEM((head_width, span), jnp.float32),
            pltpu.VMEM((4, tokens, head_width), kind),
            pltpu.VMEM((2 * head_groups, rows, head_width), kind),
            pltpu.VMEM((2 * head_groups, head_width, width), kind),
            pltpu.VMEM((rows, width), jnp.float32),
            pltpu.VMEM((rows, width), kind),
            pltpu.VMEM((count, up_rows, units), kind),
            pltpu.VMEM((count, units, columns), kind),
            pltpu.VMEM((2, group, rows, width), kind),
            pltpu.VMEM((2, group, rows, units), kind),
            pltpu.VMEM(returned, kind),
            pltpu.VMEM(returned, kind),
            pltpu.VMEM(returned, kind),
            pltpu.VMEM(returned, kind),
            dma((2, head_groups)),
            dma((2, head_groups)),
            dma((2, head_groups, parts)),
            dma((2, head_groups, parts)),
            dma((2, 4)),
            dma((2, 4, 2 * head_groups)),
            dma((head_groups, 2)),
            dma((2, head_groups, 2)),
            dma((2, 2, count)),
            dma((2,)),
            dma((2, group)),
            dma((2, group)),
            dma((2, chunks)),
            dma((2, chunks, group)),
        ],
        compiler_params=pltpu.CompilerParams(
            collective_id=3, has_side_effects=True, vmem_limit_bytes=60 * 2**20
        ),
    )(
        residual,
        queries_narrow,
        keys_narrow,
        values_narrow,
        queries_broad,
        keys_broad,
        values_broad,
        gates_narrow,
        gates_broad,
        norm_gain.reshape(1, -1),
        project_narrow,
        project_broad,
        up_weight,
        down_weight,
    )


def layer(*arrays):
    queries, gates_broad, down_weight = arrays[1], arrays[8], arrays[13]
    head_groups = gates_broad.shape[1]
    narrow_heads = arrays[7].shape[1] // head_groups
    fused = (
        lax.axis_size("tp") == 2
        and head_groups == 4
        and lax.axis_size("sp") == head_groups * 4
        and narrow_heads * A_DIM + B_DIM == 128
        and down_weight.shape[1] % 128 == 0
        and queries.shape[0] % 64 == 0
    )
    return fused_local(*arrays) if fused else local(*arrays)


def solution(mesh):
    return jax.shard_map(
        layer,
        mesh=mesh,
        in_specs=(
            P(("sp", "tp"), None),
            P("sp", "tp"),
            P("sp", "tp"),
            P("sp", "tp"),
            P("sp", "tp"),
            P("sp", "tp"),
            P("sp", "tp"),
            P("sp", "tp"),
            P("sp", "tp"),
            P("tp", None),
            P("tp", None),
            P(),
            P("sp", "tp"),
            P("tp", "sp"),
        ),
        out_specs=P(("sp", "tp"), None),
        check_vma=False,
    )
```

```python
import functools

import jax
import jax.numpy as jnp
from jax import lax
from jax.experimental import pallas as pl
from jax.experimental.pallas import tpu as pltpu
from jax.sharding import PartitionSpec as P

A_DIM = 32
B_DIM = 64


def rms_scaled(mixed, norm_gain):
    mixed_wide = mixed.astype(jnp.float32)
    scale = lax.rsqrt(jnp.mean(mixed_wide * mixed_wide, axis=-1, keepdims=True) + 1e-06)
    return (mixed_wide * scale * norm_gain).astype(jnp.bfloat16)


def group_size(sp_count):
    return 8 if sp_count % 8 == 0 else sp_count


def head_columns(narrow_heads):
    ranges = [(h * A_DIM, (h + 1) * A_DIM, A_DIM) for h in range(narrow_heads)]
    return ranges + [(narrow_heads * A_DIM, narrow_heads * A_DIM + B_DIM, B_DIM)]


def attend_block(ranges, block, query, kv_all, gate_all):
    tokens, width = query.shape
    lane = lax.broadcasted_iota(jnp.int32, (tokens, width), 1)
    row = lax.broadcasted_iota(jnp.int32, (tokens, tokens), 0)
    column = lax.broadcasted_iota(jnp.int32, (tokens, tokens), 1)
    inside = [(lane >= low) & (lane < high) for low, high, _ in ranges]
    wide = query.astype(jnp.float32)
    head_queries = [jnp.where(mask, wide, 0.0).astype(jnp.bfloat16) for mask in inside]
    own_gates = gate_all[block]
    query_gates = [
        jnp.sum(jnp.where(row == column, own_gates[h : h + 1, :], 0.0), axis=1, keepdims=True)
        for h in range(len(ranges))
    ]

    def by_head(columns):
        spread = jnp.broadcast_to(columns[-1], (tokens, width))
        for mask, values in zip(inside[:-1], columns[:-1]):
            spread = jnp.where(mask, values, spread)
        return spread

    def step(key_block, state):
        peaks, totals, summed = state
        keys = kv_all[key_block, :, :width]
        values = kv_all[key_block, :, width:]
        key_gates = gate_all[key_block]
        allowed = column + (key_block - block) * tokens <= row
        new_peaks, new_totals, fades, terms = [], [], [], []
        for h, (_, _, size) in enumerate(ranges):
            scores = (
                lax.dot_general(
                    head_queries[h],
                    keys,
                    (((1,), (1,)), ((), ())),
                    preferred_element_type=jnp.float32,
                )
                * size ** (-0.5)
                + query_gates[h]
                - key_gates[h : h + 1, :]
            )
            scores = jnp.where(allowed, scores, -1e30)
            peak = jnp.maximum(peaks[h], jnp.max(scores, axis=1, keepdims=True))
            weights = jnp.exp(scores - peak)
            fade = jnp.exp(peaks[h] - peak)
            new_peaks.append(peak)
            new_totals.append(totals[h] * fade + jnp.sum(weights, axis=1, keepdims=True))
            fades.append(fade)
            terms.append(
                jnp.dot(
                    weights.astype(jnp.bfloat16), values, preferred_element_type=jnp.float32
                )
            )
        summed = summed * by_head(fades) + by_head(terms)
        return tuple(new_peaks), tuple(new_totals), summed

    heads = len(ranges)
    initial = (
        tuple(jnp.full((tokens, 1), -1e30, jnp.float32) for _ in range(heads)),
        tuple(jnp.zeros((tokens, 1), jnp.float32) for _ in range(heads)),
        jnp.zeros((tokens, width), jnp.float32),
    )
    _, totals, summed = lax.fori_loop(0, block + 1, step, initial)
    return (summed / by_head(totals)).astype(jnp.bfloat16)


def layer_kernel(
    count,
    group,
    ranges,
    q_ref,
    kv_ref,
    gate_ref,
    up_ref,
    down_ref,
    attended_out,
    up_out,
    down_out,
    q_all,
    kv_all,
    gate_all,
    attended,
    up_hold,
    down_hold,
    kv_sems,
    gate_sems,
    q_sems,
    back_sems,
    sems,
    own_sems,
):
    me = lax.axis_index("sp")
    head_groups = q_ref.shape[0]
    parts = count // head_groups
    my_heads = me % head_groups
    my_part = me // head_groups

    def block_of(part, slot):
        turn = slot % 2
        return slot * parts + (1 - turn) * part + turn * (parts - 1 - part)

    my_slot = me // parts
    my_turn = my_slot % 2
    place = me % parts
    reader_part = (1 - my_turn) * place + my_turn * (parts - 1 - place)
    up_rows = up_ref.shape[0]
    units = up_out.shape[1]
    columns = down_ref.shape[1]
    barrier = pltpu.get_barrier_semaphore()

    def hello(k, carry):
        pl.semaphore_signal(
            barrier,
            inc=1,
            device_id={"sp": (me + k) % count},
            device_id_type=pl.DeviceIdType.MESH,
        )
        return carry

    lax.fori_loop(1, count, hello, 0)
    pl.semaphore_wait(barrier, count - 1)

    def remote(source, target, sem_pair, first, second, peer):
        return pltpu.make_async_remote_copy(
            src_ref=source,
            dst_ref=target,
            send_sem=sem_pair.at[0, first],
            recv_sem=sem_pair.at[1, second],
            device_id={"sp": peer},
            device_id_type=pl.DeviceIdType.MESH,
        )

    def context_copies(k, owner):
        peer = (me + k) % count
        heads = peer % head_groups
        return (
            remote(kv_ref.at[heads], kv_all.at[owner], kv_sems, k, k, peer),
            remote(gate_ref.at[heads], gate_all.at[owner], gate_sems, k, k, peer),
        )

    def start_context(k, carry):
        for copy in context_copies(k, me):
            copy.start()
        return carry

    def wait_context(k, carry):
        for copy in context_copies(k, (me + count - k) % count):
            copy.wait_recv()
            copy.wait_send()
        return carry

    for heads in range(head_groups):
        reader = reader_part * head_groups + heads

        @pl.when(reader != me)
        def _():
            remote(q_ref.at[heads], q_all.at[my_slot], q_sems, heads, my_slot, reader).start()

        @pl.when(reader == me)
        def _():
            q_all[my_slot] = q_ref[heads]

    lax.fori_loop(1, count, start_context, 0)
    kv_all[me] = kv_ref[my_heads]
    gate_all[me] = gate_ref[my_heads]

    def up_source(chunk):
        return up_ref.at[:, pl.ds(pl.multiple_of(chunk * units, 128), units)]

    def down_source(chunk):
        return down_ref.at[pl.ds(pl.multiple_of(chunk * units, units), units), :]

    def up_target(owner):
        return up_out.at[pl.ds(pl.multiple_of(owner * up_rows, up_rows), up_rows), :]

    def down_target(owner):
        if len(down_out.shape) == 3:
            return down_out.at[owner]
        return down_out.at[:, pl.ds(pl.multiple_of(owner * columns, columns), columns)]

    def copies(k, target_owner):
        peer = (me + k) % count
        chunk = peer % group
        pairs = (
            (up_source(chunk), up_target(target_owner)),
            (down_source(chunk), down_target(target_owner)),
        )
        return [
            pltpu.make_async_remote_copy(
                src_ref=source,
                dst_ref=target,
                send_sem=sems.at[0, which, k],
                recv_sem=sems.at[1, which, k],
                device_id={"sp": peer},
                device_id_type=pl.DeviceIdType.MESH,
            )
            for which, (source, target) in enumerate(pairs)
        ]

    def start(k, carry):
        for copy in copies(k, me):
            copy.start()
        return carry

    def finish(k, carry):
        for copy in copies(k, (me + count - k) % count):
            copy.wait_recv()
            copy.wait_send()
        return carry

    lax.fori_loop(1, count, start, 0)
    own = me % group
    first = [
        pltpu.make_async_copy(up_source(own), up_hold, own_sems.at[0]),
        pltpu.make_async_copy(down_source(own), down_hold, own_sems.at[1]),
    ]
    for copy in first:
        copy.start()
    for copy in first:
        copy.wait()
    second = [
        pltpu.make_async_copy(up_hold, up_target(me), own_sems.at[0]),
        pltpu.make_async_copy(down_hold, down_target(me), own_sems.at[1]),
    ]
    for copy in second:
        copy.start()
    for heads in range(head_groups):
        reader = reader_part * head_groups + heads

        @pl.when(reader != me)
        def _():
            remote(q_ref.at[heads], q_all.at[my_slot], q_sems, heads, my_slot, reader).wait_send()

    for slot in range(head_groups):
        owner = block_of(my_part, slot)

        @pl.when(owner != me)
        def _():
            remote(q_ref.at[0], q_all.at[slot], q_sems, 0, slot, owner).wait_recv()

    lax.fori_loop(1, count, wait_context, 0)

    def attend(slot, carry):
        block = block_of(my_part, slot)
        attended[slot] = attend_block(ranges, block, q_all[slot], kv_all, gate_all)
        return carry

    lax.fori_loop(0, head_groups, attend, 0)
    for slot in range(head_groups):
        owner = block_of(my_part, slot)

        @pl.when(owner != me)
        def _():
            remote(
                attended.at[slot], attended_out.at[my_heads], back_sems, slot, my_heads, owner
            ).start()

        @pl.when(owner == me)
        def _():
            attended_out[my_heads] = attended[slot]

    for copy in second:
        copy.wait()
    lax.fori_loop(1, count, finish, 0)
    for slot in range(head_groups):
        owner = block_of(my_part, slot)

        @pl.when(owner != me)
        def _():
            remote(
                attended.at[slot], attended_out.at[my_heads], back_sems, slot, my_heads, owner
            ).wait_send()

    for heads in range(head_groups):
        reader = reader_part * head_groups + heads

        @pl.when(reader != me)
        def _():
            remote(
                attended.at[0], attended_out.at[heads], back_sems, 0, heads, reader
            ).wait_recv()


def attend_and_share(queries, keys_values, gates, ranges, up_weight, down_weight):
    head_groups, tokens, head_width = queries.shape
    count = lax.axis_size("sp")
    group = group_size(count)
    up_rows, unit_total = up_weight.shape
    columns = down_weight.shape[1]
    units = unit_total // group
    if columns % 128 == 0:
        down_shape = (units, count * columns)
    else:
        down_shape = (count, units, columns)
    attended, up_full, down_full = pl.pallas_call(
        functools.partial(layer_kernel, count, group, ranges),
        out_shape=(
            jax.ShapeDtypeStruct(queries.shape, queries.dtype),
            jax.ShapeDtypeStruct((count * up_rows, units), up_weight.dtype),
            jax.ShapeDtypeStruct(down_shape, down_weight.dtype),
        ),
        in_specs=[pl.BlockSpec(memory_space=pltpu.VMEM)] * 3
        + [pl.BlockSpec(memory_space=pl.ANY)] * 2,
        out_specs=[pl.BlockSpec(memory_space=pltpu.VMEM)]
        + [pl.BlockSpec(memory_space=pl.ANY)] * 2,
        scratch_shapes=[
            pltpu.VMEM(queries.shape, queries.dtype),
            pltpu.VMEM((count,) + keys_values.shape[1:], keys_values.dtype),
            pltpu.VMEM((count,) + gates.shape[1:], gates.dtype),
            pltpu.VMEM(queries.shape, queries.dtype),
            pltpu.VMEM((up_rows, units), up_weight.dtype),
            pltpu.VMEM((units, columns), down_weight.dtype),
            pltpu.SemaphoreType.DMA((2, count)),
            pltpu.SemaphoreType.DMA((2, count)),
            pltpu.SemaphoreType.DMA((2, head_groups)),
            pltpu.SemaphoreType.DMA((2, head_groups)),
            pltpu.SemaphoreType.DMA((2, 2, count)),
            pltpu.SemaphoreType.DMA((2,)),
        ],
        compiler_params=pltpu.CompilerParams(collective_id=0, has_side_effects=True),
        cost_estimate=pl.CostEstimate(
            flops=0, bytes_accessed=count * up_rows * units * 80, transcendentals=0
        ),
    )(queries, keys_values, gates, up_weight, down_weight)
    if columns % 128:
        down_full = down_full.transpose(1, 0, 2).reshape(units, count * columns)
    return attended, up_full, down_full


def gather_kernel(group, tp_count, rows_ref, out_ref, hold, sems, own_sems, pass_sems):
    sp = lax.axis_index("sp")
    tp = lax.axis_index("tp")
    base = (sp // group) * group
    me = sp - base
    barrier = pltpu.get_barrier_semaphore()
    for k in range(1, group):
        pl.semaphore_signal(
            barrier,
            inc=1,
            device_id={"sp": base + (me + k) % group},
            device_id_type=pl.DeviceIdType.MESH,
        )
    for j in range(1, tp_count):
        pl.semaphore_signal(
            barrier,
            inc=1,
            device_id={"tp": (tp + j) % tp_count},
            device_id_type=pl.DeviceIdType.MESH,
        )
    pl.semaphore_wait(barrier, group + tp_count - 2)

    def across(k, owner):
        return pltpu.make_async_remote_copy(
            src_ref=rows_ref,
            dst_ref=out_ref.at[tp, owner],
            send_sem=sems.at[0, k],
            recv_sem=sems.at[1, k],
            device_id={"sp": base + (me + k) % group},
            device_id_type=pl.DeviceIdType.MESH,
        )

    def beside(j, k, source, tp_owner, owner):
        return pltpu.make_async_remote_copy(
            src_ref=source,
            dst_ref=out_ref.at[tp_owner, owner],
            send_sem=pass_sems.at[0, j, k],
            recv_sem=pass_sems.at[1, j, k],
            device_id={"tp": (tp + j) % tp_count},
            device_id_type=pl.DeviceIdType.MESH,
        )

    for k in range(1, group):
        across(k, me).start()
    for j in range(1, tp_count):
        beside(j, 0, rows_ref, tp, me).start()
    own = pltpu.make_async_copy(rows_ref, hold, own_sems.at[0])
    own.start()
    own.wait()
    own = pltpu.make_async_copy(hold, out_ref.at[tp, me], own_sems.at[1])
    own.start()
    own.wait()
    for k in range(1, group):
        owner = (me + group - k) % group
        across(k, owner).wait_recv()
        for j in range(1, tp_count):
            beside(j, k, out_ref.at[tp, owner], tp, owner).start()
    for k in range(1, group):
        across(k, me).wait_send()
    for j in range(1, tp_count):
        for k in range(group):
            owner = (me + group - k) % group
            copy = beside(j, k, rows_ref, (tp + tp_count - j) % tp_count, owner)
            copy.wait_send()
            copy.wait_recv()


def gather_rows(rows):
    group = group_size(lax.axis_size("sp"))
    tp_count = lax.axis_size("tp")
    return pl.pallas_call(
        functools.partial(gather_kernel, group, tp_count),
        out_shape=jax.ShapeDtypeStruct((tp_count, group) + rows.shape, rows.dtype),
        in_specs=[pl.BlockSpec(memory_space=pl.ANY)],
        out_specs=pl.BlockSpec(memory_space=pl.ANY),
        scratch_shapes=[
            pltpu.VMEM(rows.shape, rows.dtype),
            pltpu.SemaphoreType.DMA((2, group)),
            pltpu.SemaphoreType.DMA((2,)),
            pltpu.SemaphoreType.DMA((2, tp_count, group)),
        ],
        compiler_params=pltpu.CompilerParams(collective_id=1, has_side_effects=True),
    )(rows)


def return_kernel(group, parts_ref, out_ref, hold, sems, own_sems):
    sp = lax.axis_index("sp")
    base = (sp // group) * group
    me = sp - base
    barrier = pltpu.get_barrier_semaphore()
    for k in range(1, group):
        pl.semaphore_signal(
            barrier,
            inc=1,
            device_id={"sp": base + (me + k) % group},
            device_id_type=pl.DeviceIdType.MESH,
        )
    pl.semaphore_wait(barrier, group - 1)

    def across(k, owner):
        peer = (me + k) % group
        return pltpu.make_async_remote_copy(
            src_ref=parts_ref.at[peer],
            dst_ref=out_ref.at[owner],
            send_sem=sems.at[0, k],
            recv_sem=sems.at[1, k],
            device_id={"sp": base + peer},
            device_id_type=pl.DeviceIdType.MESH,
        )

    for k in range(1, group):
        across(k, me).start()
    own = pltpu.make_async_copy(parts_ref.at[me], hold, own_sems.at[0])
    own.start()
    own.wait()
    own = pltpu.make_async_copy(hold, out_ref.at[me], own_sems.at[1])
    own.start()
    own.wait()
    for k in range(1, group):
        copy = across(k, (me + group - k) % group)
        copy.wait_recv()
        copy.wait_send()


def return_parts(parts):
    group = parts.shape[0]
    return pl.pallas_call(
        functools.partial(return_kernel, group),
        out_shape=jax.ShapeDtypeStruct(parts.shape, parts.dtype),
        in_specs=[pl.BlockSpec(memory_space=pl.ANY)],
        out_specs=pl.BlockSpec(memory_space=pl.ANY),
        scratch_shapes=[
            pltpu.VMEM(parts.shape[1:], parts.dtype),
            pltpu.SemaphoreType.DMA((2, group)),
            pltpu.SemaphoreType.DMA((2,)),
        ],
        compiler_params=pltpu.CompilerParams(collective_id=2, has_side_effects=True),
    )(parts)


def local(
    residual,
    queries_narrow,
    keys_narrow,
    values_narrow,
    queries_broad,
    keys_broad,
    values_broad,
    gates_narrow,
    gates_broad,
    project_narrow,
    project_broad,
    norm_gain,
    up_weight,
    down_weight,
):
    tokens = queries_narrow.shape[0]
    head_groups = gates_broad.shape[1]
    narrow_heads = gates_narrow.shape[1] // head_groups
    ranges = head_columns(narrow_heads)

    def by_group(narrow, broad):
        return jnp.concatenate(
            [part.reshape(tokens, head_groups, -1) for part in (narrow, broad)], axis=-1
        ).transpose(1, 0, 2)

    gates = jnp.concatenate(
        [gates_narrow.reshape(tokens, head_groups, narrow_heads), gates_broad[..., None]], axis=-1
    ).transpose(1, 2, 0)
    gates = jnp.pad(gates, ((0, 0), (0, -gates.shape[1] % 8), (0, 0)))
    attended, up_full, down_full = attend_and_share(
        by_group(queries_narrow, queries_broad),
        jnp.concatenate(
            [by_group(keys_narrow, keys_broad), by_group(values_narrow, values_broad)], axis=-1
        ),
        gates,
        ranges,
        up_weight,
        down_weight,
    )
    rows_first = attended.transpose(1, 0, 2)
    split = narrow_heads * A_DIM
    attended_narrow = rows_first[..., :split].reshape(tokens, -1)
    attended_broad = rows_first[..., split:].reshape(tokens, -1)
    projected = lax.psum_scatter(
        (
            jnp.dot(attended_narrow, project_narrow, preferred_element_type=jnp.float32)
            + jnp.dot(attended_broad, project_broad, preferred_element_type=jnp.float32)
        ).astype(jnp.bfloat16),
        "tp",
        scatter_dimension=0,
        tiled=True,
    ).astype(jnp.float32)
    mixed = (residual.astype(jnp.float32) + projected).astype(jnp.bfloat16)
    features = gather_rows(rms_scaled(mixed, norm_gain))
    tp_count, group, rows, width = features.shape
    up_total = jnp.dot(
        features.reshape(tp_count * group * rows, width),
        up_full,
        preferred_element_type=jnp.float32,
    )
    hidden = jnp.square(jax.nn.relu(up_total)).astype(jnp.bfloat16)
    down_term = jnp.dot(hidden, down_full, preferred_element_type=jnp.float32)
    parts = lax.psum_scatter(
        down_term.astype(jnp.bfloat16).reshape(features.shape),
        "tp",
        scatter_dimension=0,
        tiled=False,
    )
    summed_rows = jnp.sum(return_parts(parts).astype(jnp.float32), axis=0)
    return (mixed.astype(jnp.float32) + summed_rows).astype(jnp.bfloat16)


IN_FLIGHT = 3
LOG2E = 1.4426950408889634
PIECES = 3
GATE_ROWS = 16


def split_pieces(values):
    pieces = []
    rest = values
    for _ in range(PIECES):
        piece = rest.astype(jnp.bfloat16).astype(jnp.float32)
        pieces.append(piece)
        rest = rest - piece
    return pieces


def pad_rows(values, rows):
    return jnp.concatenate(
        [values, jnp.zeros((rows - values.shape[0], values.shape[1]), values.dtype)], axis=0
    )


def pad_lanes(values, lanes):
    return jnp.concatenate(
        [values, jnp.zeros((values.shape[0], lanes - values.shape[1]), values.dtype)], axis=1
    )


def fused_kernel(
    count,
    group,
    head_groups,
    ranges,
    residual_ref,
    qn_ref,
    kn_ref,
    vn_ref,
    qb_ref,
    kb_ref,
    vb_ref,
    gn_ref,
    gb_ref,
    gain_ref,
    pn_ref,
    pb_ref,
    up_ref,
    down_ref,
    out_ref,
    q_send,
    kv_send,
    gate_send,
    q_all,
    kv_all,
    gate_all,
    key_gates,
    v_turned,
    q_wide,
    acc,
    attended,
    attended_in,
    project,
    mixed,
    normed,
    up_all,
    down_all,
    features,
    hidden,
    part_out,
    part_in,
    return_out,
    return_in,
    kv_line,
    gate_line,
    kv_plane,
    gate_plane,
    q_sems,
    back_sems,
    project_own,
    project_sems,
    share_sems,
    twin_sems,
    own_sems,
    across_sems,
    beside_sems,
    part_sems,
    return_sems,
):
    me = lax.axis_index("sp")
    tp = lax.axis_index("tp")
    other = 1 - tp
    planes = head_groups
    parts = count // planes
    plane = me // parts
    lane = me % parts
    base = (me // group) * group
    local = me - base
    tokens, _ = qn_ref.shape
    rows, width = residual_ref.shape
    heads = len(ranges)
    head_width = q_send.shape[2]
    narrow_width = ranges[-1][0]
    broad_width = head_width - narrow_width
    span = 2 * tokens
    barrier = pltpu.get_barrier_semaphore()

    def remote(source, target, send, recv, sp, core):
        return pltpu.make_async_remote_copy(
            src_ref=source,
            dst_ref=target,
            send_sem=send,
            recv_sem=recv,
            device_id={"sp": sp, "tp": core},
            device_id_type=pl.DeviceIdType.MESH,
        )

    def hello(k, carry):
        flat = (me * 2 + tp + k) % (count * 2)
        pl.semaphore_signal(
            barrier,
            inc=1,
            device_id={"sp": flat // 2, "tp": flat % 2},
            device_id_type=pl.DeviceIdType.MESH,
        )
        return carry

    lax.fori_loop(1, count * 2, hello, 0)

    def by_group(narrow_ref, broad_ref, h):
        return [
            narrow_ref[:, h * narrow_width : (h + 1) * narrow_width],
            broad_ref[:, h * broad_width : (h + 1) * broad_width],
        ]

    narrow_heads = heads - 1
    gates = jnp.concatenate([gn_ref[...], gb_ref[...]], axis=0)
    for h in range(head_groups):
        kv_send[h] = jnp.concatenate(
            by_group(kn_ref, kb_ref, h) + by_group(vn_ref, vb_ref, h), axis=1
        )
        q_send[h] = jnp.concatenate(by_group(qn_ref, qb_ref, h), axis=1)
        lines = []
        for i, (_, _, size) in enumerate(ranges):
            if i < narrow_heads:
                source = h * narrow_heads + i
            else:
                source = head_groups * narrow_heads + h
            lines += split_pieces(gates[source : source + 1] * size**0.5)
        lines += [jnp.ones((PIECES, tokens), jnp.float32)]
        gate_send[h] = pad_rows(jnp.concatenate(lines, axis=0), GATE_ROWS).astype(jnp.bfloat16)

    pl.semaphore_wait(barrier, count * 2 - 1)

    def line_copies(j, owner):
        target = (plane + j) % planes
        peer = target * parts + lane
        return (
            remote(
                kv_send.at[target], kv_all.at[owner], kv_line.at[0, j], kv_line.at[1, j], peer, tp
            ),
            remote(
                gate_send.at[target],
                gate_all.at[owner],
                gate_line.at[0, j],
                gate_line.at[1, j],
                peer,
                tp,
            ),
        )

    def line_owner(j):
        return ((plane + planes - j) % planes) * parts + lane

    def plane_copies(j, k, kv_source, gate_source, owner):
        peer = plane * parts + (lane + k) % parts
        return (
            remote(
                kv_source,
                kv_all.at[owner],
                kv_plane.at[0, j, k],
                kv_plane.at[1, j, k],
                peer,
                tp,
            ),
            remote(
                gate_source,
                gate_all.at[owner],
                gate_plane.at[0, j, k],
                gate_plane.at[1, j, k],
                peer,
                tp,
            ),
        )

    for j in range(1, planes):
        for copy in line_copies(j, me):
            copy.start()
    for k in range(1, parts):
        for copy in plane_copies(0, k, kv_send.at[plane], gate_send.at[plane], me):
            copy.start()
    kv_all[me] = kv_send[plane]
    gate_all[me] = gate_send[plane]

    double = me // 2
    reader_part = jnp.where(double < parts, double, 2 * parts - 1 - double)
    my_slot = 2 * (double // parts) + me % 2

    def tile_double(tile):
        return tile * (2 * parts - 1 - lane) + (1 - tile) * lane

    for h in range(head_groups):
        reader = h * parts + reader_part

        @pl.when(reader != me)
        def _():
            remote(
                q_send.at[h], q_all.at[my_slot], q_sems.at[0, h], q_sems.at[1, my_slot], reader, tp
            ).start()

        @pl.when(reader == me)
        def _():
            q_all[my_slot] = q_send[h]

    def project_pairs(h):
        pairs = []
        for source, low, size in (
            (pn_ref, 0, narrow_width),
            (pb_ref, narrow_width, broad_width),
        ):
            pairs.append(
                (
                    source.at[h * size : (h + 1) * size, :],
                    project.at[tp * head_groups + h, low : low + size, :],
                )
            )
        return pairs

    def project_copies(h):
        own, away = [], []
        for i, (source, target) in enumerate(project_pairs(h)):
            own.append(pltpu.make_async_copy(source, target, project_own.at[h, i]))
            away.append(
                remote(
                    source,
                    target,
                    project_sems.at[0, h, i],
                    project_sems.at[1, h, i],
                    me,
                    other,
                )
            )
        return own, away

    for h in range(head_groups):
        own, away = project_copies(h)
        for copy in own + away:
            copy.start()

    units = up_all.shape[2]

    def up_source(chunk):
        return up_ref.at[:, pl.ds(pl.multiple_of(chunk * units, 128), units)]

    def down_source(chunk):
        return down_ref.at[pl.ds(pl.multiple_of(chunk * units, units), units), :]

    def flip(place, bit):
        return place + bit * (1 - 2 * ((place // bit) % 2))

    def mate(place, offset):
        bit = 1
        while bit <= offset:
            if offset & bit:
                place = flip(place, bit)
            bit *= 2
        return place

    def share_copy(which, offset, owner):
        peer = mate(local, offset)
        source = up_source(peer) if which == 0 else down_source(peer)
        target = up_all.at[owner] if which == 0 else down_all.at[owner]
        return remote(
            source,
            target,
            share_sems.at[0, which, offset],
            share_sems.at[1, which, offset],
            base + peer,
            tp,
        )

    twin = (me + group) % count
    twin_base = (base + group) % count

    def twin_copy(which, offset):
        owner = base + mate(local, offset)
        weights = up_all if which == 0 else down_all
        if offset:
            source = weights.at[owner]
        else:
            source = up_source(local) if which == 0 else down_source(local)
        return remote(
            source,
            weights.at[owner],
            twin_sems.at[0, which, offset],
            twin_sems.at[1, which, offset],
            twin,
            tp,
        )

    far = group // 2
    near = [offset for offset in range(1, group) if offset != far]
    near.sort(key=lambda offset: (bin(offset).count("1"), offset))
    pieces = [(0, 0), (1, 0), (0, far), (1, far)]
    pieces += [(which, offset) for which in range(2) for offset in near]
    issued = []

    def tick(amount=1):
        for _ in range(amount):
            if len(issued) == len(pieces):
                return
            which, offset = pieces[len(issued)]
            if len(issued) >= IN_FLIGHT:
                twin_copy(*pieces[len(issued) - IN_FLIGHT]).wait_send()
            if offset:
                share_copy(which, offset, base + mate(local, offset)).wait_recv()
            twin_copy(which, offset).start()
            issued.append((which, offset))

    own_weights = [
        pltpu.make_async_copy(up_source(local), up_all.at[me], own_sems.at[0]),
        pltpu.make_async_copy(down_source(local), down_all.at[me], own_sems.at[1]),
    ]
    for copy in own_weights:
        copy.start()
    for which in range(2):
        share_copy(which, far, me).start()
    tick(2)

    for j in range(1, planes):
        owner = line_owner(j)
        for copy in line_copies(j, owner):
            copy.wait_recv()
        for k in range(1, parts):
            for copy in plane_copies(j, k, kv_all.at[owner], gate_all.at[owner], owner):
                copy.start()

    for which in range(2):
        for offset in near:
            share_copy(which, offset, me).start()
    tick(2)

    for j in range(planes):
        for k in range(1, parts):
            owner = ((plane + planes - j) % planes) * parts + (lane + parts - k) % parts
            for copy in plane_copies(j, k, kv_all.at[owner], gate_all.at[owner], owner):
                copy.wait_recv()

    def turn(pair, carry):
        values = kv_all[pl.ds(2 * pair, 2), :, head_width:].reshape(span, head_width)
        v_turned[pair] = values.astype(jnp.float32).T.astype(jnp.bfloat16)
        for i in range(2):
            block = pad_rows(gate_all[2 * pair + i].astype(jnp.float32), 128)
            block = pad_lanes(block, -(-tokens // 128) * 128).T[:tokens]
            key_gates[2 * pair + i] = block.astype(jnp.bfloat16)
        return carry

    lax.fori_loop(0, count // 2, turn, 0)

    for slot in range(4):
        owner = 2 * tile_double(slot // 2) + slot % 2

        @pl.when(owner != me)
        def _():
            remote(
                q_send.at[0], q_all.at[slot], q_sems.at[0, 0], q_sems.at[1, slot], owner, tp
            ).wait_recv()

    lane_id = lax.broadcasted_iota(jnp.int32, (span, head_width), 1)
    first_one = heads * PIECES

    def attend(tile, carry):
        double_block = tile_double(tile)
        query = q_all[pl.ds(2 * tile, 2)].reshape(span, head_width).astype(jnp.float32)
        own_gates = (
            key_gates[pl.ds(2 * double_block, 2)].reshape(span, head_width).astype(jnp.float32)
        )
        for i, (low, high, _) in enumerate(ranges):
            left = jnp.where((lane_id >= low) & (lane_id < high), query, 0.0)
            moved = pltpu.roll(own_gates, first_one - i * PIECES, 1)
            right = jnp.where((lane_id >= first_one) & (lane_id < first_one + PIECES), moved, 0.0)
            right = jnp.where(
                (lane_id >= i * PIECES) & (lane_id < (i + 1) * PIECES), -1.0, right
            )
            q_wide[i] = jnp.concatenate([left, right], axis=1).astype(jnp.bfloat16)
        acc[...] = jnp.zeros_like(acc)

        def step(pair, state, masked):
            peaks, totals = state
            keys = jnp.concatenate(
                [
                    kv_all[pl.ds(2 * pair, 2), :, :head_width].reshape(span, head_width),
                    key_gates[pl.ds(2 * pair, 2)].reshape(span, head_width),
                ],
                axis=1,
            )
            new_peaks, new_totals = [], []
            for i, (low, high, size) in enumerate(ranges):
                factor = size**-0.5 * LOG2E
                scores = lax.dot_general(
                    keys, q_wide[i], (((1,), (1,)), ((), ())), preferred_element_type=jnp.float32
                )
                if masked:
                    row = lax.broadcasted_iota(jnp.int32, (span, span), 0)
                    column = lax.broadcasted_iota(jnp.int32, (span, span), 1)
                    scores = jnp.where(row <= column, scores, -1e30)
                peak = jnp.maximum(peaks[i], jnp.max(scores, axis=0, keepdims=True))
                weights = jnp.exp2((scores - peak) * factor)
                fade = jnp.exp2((peaks[i] - peak) * factor)
                new_peaks.append(peak)
                new_totals.append(totals[i] * fade + jnp.sum(weights, axis=0, keepdims=True))
                acc[low:high, :] = acc[low:high, :] * fade + jnp.dot(
                    v_turned[pair, low:high, :],
                    weights.astype(jnp.bfloat16),
                    preferred_element_type=jnp.float32,
                )
            return tuple(new_peaks), tuple(new_totals)

        state = (
            tuple(jnp.full((1, span), -1e30, jnp.float32) for _ in ranges),
            tuple(jnp.zeros((1, span), jnp.float32) for _ in ranges),
        )
        state = lax.fori_loop(
            0, double_block, lambda pair, state: step(pair, state, False), state
        )
        _, totals = step(double_block, state, True)
        scaled = jnp.concatenate(
            [acc[low:high, :] / totals[i] for i, (low, high, _) in enumerate(ranges)], axis=0
        )
        attended[pl.ds(2 * tile, 2)] = (
            scaled.T.astype(jnp.bfloat16).reshape(2, tokens, head_width)
        )
        return carry

    def back_copy(slot, core, place, sp):
        return remote(
            attended.at[slot, core * rows : (core + 1) * rows, :],
            attended_in.at[place],
            back_sems.at[0, slot, core],
            back_sems.at[1, 0, place],
            sp,
            core,
        )

    my_place = tp * head_groups + plane
    for slot in range(4):
        if slot % 2 == 0:
            attend(1 - slot // 2, 0)
            tick()
        slot = (slot + 2) % 4
        owner = 2 * tile_double(slot // 2) + slot % 2
        for core in range(2):
            here = (owner == me) & (tp == core)

            @pl.when(jnp.logical_not(here))
            def _():
                back_copy(slot, core, my_place, owner).start()

            @pl.when(here)
            def _():
                attended_in[my_place] = attended[slot, core * rows : (core + 1) * rows, :]

    tick()
    for h in range(head_groups):
        own, away = project_copies(h)
        for copy in own:
            copy.wait()
        for copy in away:
            copy.wait()
    for h in range(head_groups):
        for core in range(2):
            place = core * head_groups + h
            sender = h * parts + reader_part

            @pl.when(jnp.logical_not((sender == me) & (tp == core)))
            def _():
                remote(
                    attended.at[0, :rows, :],
                    attended_in.at[place],
                    back_sems.at[0, 0, 0],
                    back_sems.at[1, 0, place],
                    sender,
                    core,
                ).wait_recv()

    step_width = return_out.shape[3]
    chunks = width // step_width
    joined = jnp.concatenate([attended_in[i] for i in range(2 * head_groups)], axis=1)

    def project_step(n, squares):
        columns = pl.ds(pl.multiple_of(n * step_width, step_width), step_width)
        total = residual_ref[:, columns].astype(jnp.float32) + jnp.dot(
            joined,
            project[:, :, columns].reshape(2 * head_groups * head_width, step_width),
            preferred_element_type=jnp.float32,
        )
        total = total.astype(jnp.bfloat16).astype(jnp.float32)
        mixed[:, columns] = total
        return squares + jnp.sum(total * total, axis=1, keepdims=True)

    squares = lax.fori_loop(0, chunks, project_step, jnp.zeros((rows, 1), jnp.float32))
    scale = lax.rsqrt(squares / width + 1e-06)
    scaled_rows = (mixed[...] * scale * gain_ref[...]).astype(jnp.bfloat16)
    normed[...] = scaled_rows
    features[tp, local] = scaled_rows

    bits = (group // 2, 1 + tp, 2 - tp)
    levels = len(bits)

    def member(subset):
        place = local
        for level in range(levels):
            if (subset >> level) & 1:
                place = flip(place, bits[level])
        return place

    def across(subset):
        level = subset.bit_length() - 1
        held = subset - (1 << level)
        owner = member(held)
        return remote(
            features.at[tp, owner] if held else normed,
            features.at[tp, owner],
            across_sems.at[0, subset],
            across_sems.at[1, subset],
            base + flip(local, bits[level]),
            tp,
        )

    def beside(subset):
        owner = member(subset)
        return remote(
            features.at[tp, owner] if subset else normed,
            features.at[tp, owner],
            beside_sems.at[0, subset],
            beside_sems.at[1, subset],
            me,
            other,
        )

    def spread(subset):
        for level in range(subset.bit_length(), levels):
            across(subset + (1 << level)).start()
        beside(subset).start()

    spread(0)
    for subset in range(1, group):
        across(subset).wait_recv()
        spread(subset)
        tick()
    for subset in range(group):
        beside(subset).wait_recv()

    own_weights[0].wait()
    tick(len(pieces))
    for offset in range(group):
        twin_copy(0, offset).wait_recv()

    row_groups = 2
    some = group // row_groups

    def up_step(i, carry):
        core = (other + i // row_groups) % 2
        chips = pl.ds((i % row_groups) * some, some)
        total = jnp.dot(
            features[core, chips].reshape(some * rows, width),
            up_all[...].reshape(width, units),
            preferred_element_type=jnp.float32,
        )
        total = jnp.maximum(total, 0.0)
        hidden[core, chips] = (
            (total * total).astype(jnp.bfloat16).reshape(some, rows, units)
        )
        return carry

    lax.fori_loop(0, 2 * row_groups, up_step, 0)
    own_weights[1].wait()

    for offset in range(group):
        twin_copy(1, offset).wait_recv()

    per_chunk = count // chunks

    def down_columns(chunk):
        return jnp.concatenate(
            [down_all[chunk * per_chunk + i] for i in range(per_chunk)], axis=1
        )

    def part_copy(chunk):
        return remote(
            part_out.at[chunk],
            part_in.at[chunk],
            part_sems.at[0, chunk],
            part_sems.at[1, chunk],
            me,
            other,
        )

    def down_dot(core, chips, chunk):
        return jnp.dot(
            hidden[core, chips].reshape(some * rows, units),
            down_columns(chunk),
            preferred_element_type=jnp.float32,
        ).reshape(some, rows, step_width)

    def away_step(chunk, carry):
        def inner(i, carry):
            chips = pl.ds(i * some, some)
            part_out[chunk, chips] = down_dot(other, chips, chunk).astype(jnp.bfloat16)
            return carry

        lax.fori_loop(0, row_groups, inner, 0)
        part_copy(chunk).start()
        return carry

    lax.fori_loop(0, chunks, away_step, 0)

    def return_copy(chunk, subset):
        level = subset.bit_length() - 1
        return remote(
            return_out.at[chunk, member(subset)],
            return_in.at[chunk, subset],
            return_sems.at[0, chunk, subset],
            return_sems.at[1, chunk, subset],
            base + flip(local, bits[level]),
            tp,
        )

    def home_step(chunk, carry):
        part_copy(chunk).wait_recv()

        def inner(i, carry):
            chips = pl.ds(i * some, some)
            return_out[chunk, chips] = (
                down_dot(tp, chips, chunk) + part_in[chunk, chips].astype(jnp.float32)
            ).astype(jnp.bfloat16)
            return carry

        lax.fori_loop(0, row_groups, inner, 0)
        for subset in range(group // 2, group):
            return_copy(chunk, subset).start()
        return carry

    lax.fori_loop(0, chunks, home_step, 0)

    for level in range(levels - 1, 0, -1):

        def merge_step(chunk, carry):
            for held in range(1 << level):
                return_copy(chunk, held + (1 << level)).wait_recv()
                place = member(held)
                return_out[chunk, place] = (
                    return_out[chunk, place].astype(jnp.float32)
                    + return_in[chunk, held + (1 << level)].astype(jnp.float32)
                ).astype(jnp.bfloat16)
            for subset in range(1 << (level - 1), 1 << level):
                return_copy(chunk, subset).start()
            return carry

        lax.fori_loop(0, chunks, merge_step, 0)

    def final_step(chunk, carry):
        columns = pl.ds(pl.multiple_of(chunk * step_width, step_width), step_width)
        return_copy(chunk, 1).wait_recv()
        total = (
            mixed[:, columns]
            + return_out[chunk, local].astype(jnp.float32)
            + return_in[chunk, 1].astype(jnp.float32)
        )
        out_ref[:, columns] = total.astype(jnp.bfloat16)
        return carry

    lax.fori_loop(0, chunks, final_step, 0)

    for j in range(1, planes):
        for copy in line_copies(j, me):
            copy.wait_send()
    for j in range(planes):
        for k in range(1, parts):
            for copy in plane_copies(j, k, kv_send.at[plane], gate_send.at[plane], me):
                copy.wait_send()
    for h in range(head_groups):
        reader = h * parts + reader_part

        @pl.when(reader != me)
        def _():
            remote(
                q_send.at[h], q_all.at[my_slot], q_sems.at[0, h], q_sems.at[1, my_slot], reader, tp
            ).wait_send()

    for slot in range(4):
        owner = 2 * tile_double(slot // 2) + slot % 2
        for core in range(2):
            here = (owner == me) & (tp == core)

            @pl.when(jnp.logical_not(here))
            def _():
                back_copy(slot, core, my_place, owner).wait_send()

    for which in range(2):
        for offset in range(1, group):
            share_copy(which, offset, me).wait_send()
    for which, offset in pieces[-IN_FLIGHT:]:
        twin_copy(which, offset).wait_send()
    for subset in range(group):
        if subset:
            across(subset).wait_send()
        beside(subset).wait_send()

    def returns_sent(chunk, carry):
        part_copy(chunk).wait_send()
        for subset in range(1, group):
            return_copy(chunk, subset).wait_send()
        return carry

    lax.fori_loop(0, chunks, returns_sent, 0)


def fused_local(
    residual,
    queries_narrow,
    keys_narrow,
    values_narrow,
    queries_broad,
    keys_broad,
    values_broad,
    gates_narrow,
    gates_broad,
    project_narrow,
    project_broad,
    norm_gain,
    up_weight,
    down_weight,
):
    count = lax.axis_size("sp")
    group = group_size(count)
    tokens = queries_narrow.shape[0]
    rows, width = residual.shape
    head_groups = gates_broad.shape[1]
    parts = count // head_groups
    narrow_heads = gates_narrow.shape[1] // head_groups
    ranges = head_columns(narrow_heads)
    heads = len(ranges)
    head_width = ranges[-1][1]
    up_rows, unit_total = up_weight.shape
    units = unit_total // group
    columns = down_weight.shape[1]
    step_width = 4 * columns
    chunks = width // step_width
    span = 2 * tokens
    kind = residual.dtype
    vmem = pl.BlockSpec(memory_space=pltpu.VMEM)
    anywhere = pl.BlockSpec(memory_space=pl.ANY)
    dma = pltpu.SemaphoreType.DMA
    returned = (chunks, group, rows, step_width)
    return pl.pallas_call(
        functools.partial(fused_kernel, count, group, head_groups, ranges),
        out_shape=jax.ShapeDtypeStruct(residual.shape, kind),
        in_specs=[vmem] * 10 + [anywhere] * 4,
        out_specs=vmem,
        scratch_shapes=[
            pltpu.VMEM((head_groups, tokens, head_width), kind),
            pltpu.VMEM((head_groups, tokens, 2 * head_width), kind),
            pltpu.VMEM((head_groups, GATE_ROWS, tokens), kind),
            pltpu.VMEM((4, tokens, head_width), kind),
            pltpu.VMEM((count, tokens, 2 * head_width), kind),
            pltpu.VMEM((count, GATE_ROWS, tokens), kind),
            pltpu.VMEM((count, tokens, head_width), kind),
            pltpu.VMEM((count // 2, head_width, span), kind),
            pltpu.VMEM((heads, span, 2 * head_width), kind),
            pltpu.VMEM((head_width, span), jnp.float32),
            pltpu.VMEM((4, tokens, head_width), kind),
            pltpu.VMEM((2 * head_groups, rows, head_width), kind),
            pltpu.VMEM((2 * head_groups, head_width, width), kind),
            pltpu.VMEM((rows, width), jnp.float32),
            pltpu.VMEM((rows, width), kind),
            pltpu.VMEM((count, up_rows, units), kind),
            pltpu.VMEM((count, units, columns), kind),
            pltpu.VMEM((2, group, rows, width), kind),
            pltpu.VMEM((2, group, rows, units), kind),
            pltpu.VMEM(returned, kind),
            pltpu.VMEM(returned, kind),
            pltpu.VMEM(returned, kind),
            pltpu.VMEM(returned, kind),
            dma((2, head_groups)),
            dma((2, head_groups)),
            dma((2, head_groups, parts)),
            dma((2, head_groups, parts)),
            dma((2, 4)),
            dma((2, 4, 2 * head_groups)),
            dma((head_groups, 2)),
            dma((2, head_groups, 2)),
            dma((2, 2, group)),
            dma((2, 2, group)),
            dma((2,)),
            dma((2, group)),
            dma((2, group)),
            dma((2, chunks)),
            dma((2, chunks, group)),
        ],
        compiler_params=pltpu.CompilerParams(
            collective_id=3, has_side_effects=True, vmem_limit_bytes=60 * 2**20
        ),
    )(
        residual,
        queries_narrow,
        keys_narrow,
        values_narrow,
        queries_broad,
        keys_broad,
        values_broad,
        gates_narrow.T,
        gates_broad.T,
        norm_gain.reshape(1, -1),
        project_narrow,
        project_broad,
        up_weight,
        down_weight,
    )


def layer(*arrays):
    queries, gates_broad, down_weight = arrays[1], arrays[8], arrays[13]
    head_groups = gates_broad.shape[1]
    narrow_heads = arrays[7].shape[1] // head_groups
    fused = (
        lax.axis_size("tp") == 2
        and head_groups == 4
        and lax.axis_size("sp") == head_groups * 4
        and group_size(lax.axis_size("sp")) == 8
        and narrow_heads * A_DIM + B_DIM == 128
        and down_weight.shape[1] % 128 == 0
        and queries.shape[0] % 64 == 0
    )
    return fused_local(*arrays) if fused else local(*arrays)


def solution(mesh):
    return jax.shard_map(
        layer,
        mesh=mesh,
        in_specs=(
            P(("sp", "tp"), None),
            P("sp", "tp"),
            P("sp", "tp"),
            P("sp", "tp"),
            P("sp", "tp"),
            P("sp", "tp"),
            P("sp", "tp"),
            P("sp", "tp"),
            P("sp", "tp"),
            P("tp", None),
            P("tp", None),
            P(),
            P("sp", "tp"),
            P("tp", "sp"),
        ),
        out_specs=P(("sp", "tp"), None),
        check_vma=False,
    )
```

```python
import functools

import jax
import jax.numpy as jnp
from jax import lax
from jax.experimental import pallas as pl
from jax.experimental.pallas import tpu as pltpu
from jax.sharding import PartitionSpec as P

A_DIM = 32
B_DIM = 64


def rms_scaled(mixed, norm_gain):
    mixed_wide = mixed.astype(jnp.float32)
    scale = lax.rsqrt(jnp.mean(mixed_wide * mixed_wide, axis=-1, keepdims=True) + 1e-06)
    return (mixed_wide * scale * norm_gain).astype(jnp.bfloat16)


def group_size(sp_count):
    return 8 if sp_count % 8 == 0 else sp_count


def head_columns(narrow_heads):
    ranges = [(h * A_DIM, (h + 1) * A_DIM, A_DIM) for h in range(narrow_heads)]
    return ranges + [(narrow_heads * A_DIM, narrow_heads * A_DIM + B_DIM, B_DIM)]


def attend_block(ranges, block, query, kv_all, gate_all):
    tokens, width = query.shape
    lane = lax.broadcasted_iota(jnp.int32, (tokens, width), 1)
    row = lax.broadcasted_iota(jnp.int32, (tokens, tokens), 0)
    column = lax.broadcasted_iota(jnp.int32, (tokens, tokens), 1)
    inside = [(lane >= low) & (lane < high) for low, high, _ in ranges]
    wide = query.astype(jnp.float32)
    head_queries = [jnp.where(mask, wide, 0.0).astype(jnp.bfloat16) for mask in inside]
    own_gates = gate_all[block]
    query_gates = [
        jnp.sum(jnp.where(row == column, own_gates[h : h + 1, :], 0.0), axis=1, keepdims=True)
        for h in range(len(ranges))
    ]

    def by_head(columns):
        spread = jnp.broadcast_to(columns[-1], (tokens, width))
        for mask, values in zip(inside[:-1], columns[:-1]):
            spread = jnp.where(mask, values, spread)
        return spread

    def step(key_block, state):
        peaks, totals, summed = state
        keys = kv_all[key_block, :, :width]
        values = kv_all[key_block, :, width:]
        key_gates = gate_all[key_block]
        allowed = column + (key_block - block) * tokens <= row
        new_peaks, new_totals, fades, terms = [], [], [], []
        for h, (_, _, size) in enumerate(ranges):
            scores = (
                lax.dot_general(
                    head_queries[h],
                    keys,
                    (((1,), (1,)), ((), ())),
                    preferred_element_type=jnp.float32,
                )
                * size ** (-0.5)
                + query_gates[h]
                - key_gates[h : h + 1, :]
            )
            scores = jnp.where(allowed, scores, -1e30)
            peak = jnp.maximum(peaks[h], jnp.max(scores, axis=1, keepdims=True))
            weights = jnp.exp(scores - peak)
            fade = jnp.exp(peaks[h] - peak)
            new_peaks.append(peak)
            new_totals.append(totals[h] * fade + jnp.sum(weights, axis=1, keepdims=True))
            fades.append(fade)
            terms.append(
                jnp.dot(
                    weights.astype(jnp.bfloat16), values, preferred_element_type=jnp.float32
                )
            )
        summed = summed * by_head(fades) + by_head(terms)
        return tuple(new_peaks), tuple(new_totals), summed

    heads = len(ranges)
    initial = (
        tuple(jnp.full((tokens, 1), -1e30, jnp.float32) for _ in range(heads)),
        tuple(jnp.zeros((tokens, 1), jnp.float32) for _ in range(heads)),
        jnp.zeros((tokens, width), jnp.float32),
    )
    _, totals, summed = lax.fori_loop(0, block + 1, step, initial)
    return (summed / by_head(totals)).astype(jnp.bfloat16)


def layer_kernel(
    count,
    group,
    ranges,
    q_ref,
    kv_ref,
    gate_ref,
    up_ref,
    down_ref,
    attended_out,
    up_out,
    down_out,
    q_all,
    kv_all,
    gate_all,
    attended,
    up_hold,
    down_hold,
    kv_sems,
    gate_sems,
    q_sems,
    back_sems,
    sems,
    own_sems,
):
    me = lax.axis_index("sp")
    head_groups = q_ref.shape[0]
    parts = count // head_groups
    my_heads = me % head_groups
    my_part = me // head_groups

    def block_of(part, slot):
        turn = slot % 2
        return slot * parts + (1 - turn) * part + turn * (parts - 1 - part)

    my_slot = me // parts
    my_turn = my_slot % 2
    place = me % parts
    reader_part = (1 - my_turn) * place + my_turn * (parts - 1 - place)
    up_rows = up_ref.shape[0]
    units = up_out.shape[1]
    columns = down_ref.shape[1]
    barrier = pltpu.get_barrier_semaphore()

    def hello(k, carry):
        pl.semaphore_signal(
            barrier,
            inc=1,
            device_id={"sp": (me + k) % count},
            device_id_type=pl.DeviceIdType.MESH,
        )
        return carry

    lax.fori_loop(1, count, hello, 0)
    pl.semaphore_wait(barrier, count - 1)

    def remote(source, target, sem_pair, first, second, peer):
        return pltpu.make_async_remote_copy(
            src_ref=source,
            dst_ref=target,
            send_sem=sem_pair.at[0, first],
            recv_sem=sem_pair.at[1, second],
            device_id={"sp": peer},
            device_id_type=pl.DeviceIdType.MESH,
        )

    def context_copies(k, owner):
        peer = (me + k) % count
        heads = peer % head_groups
        return (
            remote(kv_ref.at[heads], kv_all.at[owner], kv_sems, k, k, peer),
            remote(gate_ref.at[heads], gate_all.at[owner], gate_sems, k, k, peer),
        )

    def start_context(k, carry):
        for copy in context_copies(k, me):
            copy.start()
        return carry

    def wait_context(k, carry):
        for copy in context_copies(k, (me + count - k) % count):
            copy.wait_recv()
            copy.wait_send()
        return carry

    for heads in range(head_groups):
        reader = reader_part * head_groups + heads

        @pl.when(reader != me)
        def _():
            remote(q_ref.at[heads], q_all.at[my_slot], q_sems, heads, my_slot, reader).start()

        @pl.when(reader == me)
        def _():
            q_all[my_slot] = q_ref[heads]

    lax.fori_loop(1, count, start_context, 0)
    kv_all[me] = kv_ref[my_heads]
    gate_all[me] = gate_ref[my_heads]

    def up_source(chunk):
        return up_ref.at[:, pl.ds(pl.multiple_of(chunk * units, 128), units)]

    def down_source(chunk):
        return down_ref.at[pl.ds(pl.multiple_of(chunk * units, units), units), :]

    def up_target(owner):
        return up_out.at[pl.ds(pl.multiple_of(owner * up_rows, up_rows), up_rows), :]

    def down_target(owner):
        if len(down_out.shape) == 3:
            return down_out.at[owner]
        return down_out.at[:, pl.ds(pl.multiple_of(owner * columns, columns), columns)]

    def copies(k, target_owner):
        peer = (me + k) % count
        chunk = peer % group
        pairs = (
            (up_source(chunk), up_target(target_owner)),
            (down_source(chunk), down_target(target_owner)),
        )
        return [
            pltpu.make_async_remote_copy(
                src_ref=source,
                dst_ref=target,
                send_sem=sems.at[0, which, k],
                recv_sem=sems.at[1, which, k],
                device_id={"sp": peer},
                device_id_type=pl.DeviceIdType.MESH,
            )
            for which, (source, target) in enumerate(pairs)
        ]

    def start(k, carry):
        for copy in copies(k, me):
            copy.start()
        return carry

    def finish(k, carry):
        for copy in copies(k, (me + count - k) % count):
            copy.wait_recv()
            copy.wait_send()
        return carry

    lax.fori_loop(1, count, start, 0)
    own = me % group
    first = [
        pltpu.make_async_copy(up_source(own), up_hold, own_sems.at[0]),
        pltpu.make_async_copy(down_source(own), down_hold, own_sems.at[1]),
    ]
    for copy in first:
        copy.start()
    for copy in first:
        copy.wait()
    second = [
        pltpu.make_async_copy(up_hold, up_target(me), own_sems.at[0]),
        pltpu.make_async_copy(down_hold, down_target(me), own_sems.at[1]),
    ]
    for copy in second:
        copy.start()
    for heads in range(head_groups):
        reader = reader_part * head_groups + heads

        @pl.when(reader != me)
        def _():
            remote(q_ref.at[heads], q_all.at[my_slot], q_sems, heads, my_slot, reader).wait_send()

    for slot in range(head_groups):
        owner = block_of(my_part, slot)

        @pl.when(owner != me)
        def _():
            remote(q_ref.at[0], q_all.at[slot], q_sems, 0, slot, owner).wait_recv()

    lax.fori_loop(1, count, wait_context, 0)

    def attend(slot, carry):
        block = block_of(my_part, slot)
        attended[slot] = attend_block(ranges, block, q_all[slot], kv_all, gate_all)
        return carry

    lax.fori_loop(0, head_groups, attend, 0)
    for slot in range(head_groups):
        owner = block_of(my_part, slot)

        @pl.when(owner != me)
        def _():
            remote(
                attended.at[slot], attended_out.at[my_heads], back_sems, slot, my_heads, owner
            ).start()

        @pl.when(owner == me)
        def _():
            attended_out[my_heads] = attended[slot]

    for copy in second:
        copy.wait()
    lax.fori_loop(1, count, finish, 0)
    for slot in range(head_groups):
        owner = block_of(my_part, slot)

        @pl.when(owner != me)
        def _():
            remote(
                attended.at[slot], attended_out.at[my_heads], back_sems, slot, my_heads, owner
            ).wait_send()

    for heads in range(head_groups):
        reader = reader_part * head_groups + heads

        @pl.when(reader != me)
        def _():
            remote(
                attended.at[0], attended_out.at[heads], back_sems, 0, heads, reader
            ).wait_recv()


def attend_and_share(queries, keys_values, gates, ranges, up_weight, down_weight):
    head_groups, tokens, head_width = queries.shape
    count = lax.axis_size("sp")
    group = group_size(count)
    up_rows, unit_total = up_weight.shape
    columns = down_weight.shape[1]
    units = unit_total // group
    if columns % 128 == 0:
        down_shape = (units, count * columns)
    else:
        down_shape = (count, units, columns)
    attended, up_full, down_full = pl.pallas_call(
        functools.partial(layer_kernel, count, group, ranges),
        out_shape=(
            jax.ShapeDtypeStruct(queries.shape, queries.dtype),
            jax.ShapeDtypeStruct((count * up_rows, units), up_weight.dtype),
            jax.ShapeDtypeStruct(down_shape, down_weight.dtype),
        ),
        in_specs=[pl.BlockSpec(memory_space=pltpu.VMEM)] * 3
        + [pl.BlockSpec(memory_space=pl.ANY)] * 2,
        out_specs=[pl.BlockSpec(memory_space=pltpu.VMEM)]
        + [pl.BlockSpec(memory_space=pl.ANY)] * 2,
        scratch_shapes=[
            pltpu.VMEM(queries.shape, queries.dtype),
            pltpu.VMEM((count,) + keys_values.shape[1:], keys_values.dtype),
            pltpu.VMEM((count,) + gates.shape[1:], gates.dtype),
            pltpu.VMEM(queries.shape, queries.dtype),
            pltpu.VMEM((up_rows, units), up_weight.dtype),
            pltpu.VMEM((units, columns), down_weight.dtype),
            pltpu.SemaphoreType.DMA((2, count)),
            pltpu.SemaphoreType.DMA((2, count)),
            pltpu.SemaphoreType.DMA((2, head_groups)),
            pltpu.SemaphoreType.DMA((2, head_groups)),
            pltpu.SemaphoreType.DMA((2, 2, count)),
            pltpu.SemaphoreType.DMA((2,)),
        ],
        compiler_params=pltpu.CompilerParams(collective_id=0, has_side_effects=True),
        cost_estimate=pl.CostEstimate(
            flops=0, bytes_accessed=count * up_rows * units * 80, transcendentals=0
        ),
    )(queries, keys_values, gates, up_weight, down_weight)
    if columns % 128:
        down_full = down_full.transpose(1, 0, 2).reshape(units, count * columns)
    return attended, up_full, down_full


def gather_kernel(group, tp_count, rows_ref, out_ref, hold, sems, own_sems, pass_sems):
    sp = lax.axis_index("sp")
    tp = lax.axis_index("tp")
    base = (sp // group) * group
    me = sp - base
    barrier = pltpu.get_barrier_semaphore()
    for k in range(1, group):
        pl.semaphore_signal(
            barrier,
            inc=1,
            device_id={"sp": base + (me + k) % group},
            device_id_type=pl.DeviceIdType.MESH,
        )
    for j in range(1, tp_count):
        pl.semaphore_signal(
            barrier,
            inc=1,
            device_id={"tp": (tp + j) % tp_count},
            device_id_type=pl.DeviceIdType.MESH,
        )
    pl.semaphore_wait(barrier, group + tp_count - 2)

    def across(k, owner):
        return pltpu.make_async_remote_copy(
            src_ref=rows_ref,
            dst_ref=out_ref.at[tp, owner],
            send_sem=sems.at[0, k],
            recv_sem=sems.at[1, k],
            device_id={"sp": base + (me + k) % group},
            device_id_type=pl.DeviceIdType.MESH,
        )

    def beside(j, k, source, tp_owner, owner):
        return pltpu.make_async_remote_copy(
            src_ref=source,
            dst_ref=out_ref.at[tp_owner, owner],
            send_sem=pass_sems.at[0, j, k],
            recv_sem=pass_sems.at[1, j, k],
            device_id={"tp": (tp + j) % tp_count},
            device_id_type=pl.DeviceIdType.MESH,
        )

    for k in range(1, group):
        across(k, me).start()
    for j in range(1, tp_count):
        beside(j, 0, rows_ref, tp, me).start()
    own = pltpu.make_async_copy(rows_ref, hold, own_sems.at[0])
    own.start()
    own.wait()
    own = pltpu.make_async_copy(hold, out_ref.at[tp, me], own_sems.at[1])
    own.start()
    own.wait()
    for k in range(1, group):
        owner = (me + group - k) % group
        across(k, owner).wait_recv()
        for j in range(1, tp_count):
            beside(j, k, out_ref.at[tp, owner], tp, owner).start()
    for k in range(1, group):
        across(k, me).wait_send()
    for j in range(1, tp_count):
        for k in range(group):
            owner = (me + group - k) % group
            copy = beside(j, k, rows_ref, (tp + tp_count - j) % tp_count, owner)
            copy.wait_send()
            copy.wait_recv()


def gather_rows(rows):
    group = group_size(lax.axis_size("sp"))
    tp_count = lax.axis_size("tp")
    return pl.pallas_call(
        functools.partial(gather_kernel, group, tp_count),
        out_shape=jax.ShapeDtypeStruct((tp_count, group) + rows.shape, rows.dtype),
        in_specs=[pl.BlockSpec(memory_space=pl.ANY)],
        out_specs=pl.BlockSpec(memory_space=pl.ANY),
        scratch_shapes=[
            pltpu.VMEM(rows.shape, rows.dtype),
            pltpu.SemaphoreType.DMA((2, group)),
            pltpu.SemaphoreType.DMA((2,)),
            pltpu.SemaphoreType.DMA((2, tp_count, group)),
        ],
        compiler_params=pltpu.CompilerParams(collective_id=1, has_side_effects=True),
    )(rows)


def return_kernel(group, parts_ref, out_ref, hold, sems, own_sems):
    sp = lax.axis_index("sp")
    base = (sp // group) * group
    me = sp - base
    barrier = pltpu.get_barrier_semaphore()
    for k in range(1, group):
        pl.semaphore_signal(
            barrier,
            inc=1,
            device_id={"sp": base + (me + k) % group},
            device_id_type=pl.DeviceIdType.MESH,
        )
    pl.semaphore_wait(barrier, group - 1)

    def across(k, owner):
        peer = (me + k) % group
        return pltpu.make_async_remote_copy(
            src_ref=parts_ref.at[peer],
            dst_ref=out_ref.at[owner],
            send_sem=sems.at[0, k],
            recv_sem=sems.at[1, k],
            device_id={"sp": base + peer},
            device_id_type=pl.DeviceIdType.MESH,
        )

    for k in range(1, group):
        across(k, me).start()
    own = pltpu.make_async_copy(parts_ref.at[me], hold, own_sems.at[0])
    own.start()
    own.wait()
    own = pltpu.make_async_copy(hold, out_ref.at[me], own_sems.at[1])
    own.start()
    own.wait()
    for k in range(1, group):
        copy = across(k, (me + group - k) % group)
        copy.wait_recv()
        copy.wait_send()


def return_parts(parts):
    group = parts.shape[0]
    return pl.pallas_call(
        functools.partial(return_kernel, group),
        out_shape=jax.ShapeDtypeStruct(parts.shape, parts.dtype),
        in_specs=[pl.BlockSpec(memory_space=pl.ANY)],
        out_specs=pl.BlockSpec(memory_space=pl.ANY),
        scratch_shapes=[
            pltpu.VMEM(parts.shape[1:], parts.dtype),
            pltpu.SemaphoreType.DMA((2, group)),
            pltpu.SemaphoreType.DMA((2,)),
        ],
        compiler_params=pltpu.CompilerParams(collective_id=2, has_side_effects=True),
    )(parts)


def local(
    residual,
    queries_narrow,
    keys_narrow,
    values_narrow,
    queries_broad,
    keys_broad,
    values_broad,
    gates_narrow,
    gates_broad,
    project_narrow,
    project_broad,
    norm_gain,
    up_weight,
    down_weight,
):
    tokens = queries_narrow.shape[0]
    head_groups = gates_broad.shape[1]
    narrow_heads = gates_narrow.shape[1] // head_groups
    ranges = head_columns(narrow_heads)

    def by_group(narrow, broad):
        return jnp.concatenate(
            [part.reshape(tokens, head_groups, -1) for part in (narrow, broad)], axis=-1
        ).transpose(1, 0, 2)

    gates = jnp.concatenate(
        [gates_narrow.reshape(tokens, head_groups, narrow_heads), gates_broad[..., None]], axis=-1
    ).transpose(1, 2, 0)
    gates = jnp.pad(gates, ((0, 0), (0, -gates.shape[1] % 8), (0, 0)))
    attended, up_full, down_full = attend_and_share(
        by_group(queries_narrow, queries_broad),
        jnp.concatenate(
            [by_group(keys_narrow, keys_broad), by_group(values_narrow, values_broad)], axis=-1
        ),
        gates,
        ranges,
        up_weight,
        down_weight,
    )
    rows_first = attended.transpose(1, 0, 2)
    split = narrow_heads * A_DIM
    attended_narrow = rows_first[..., :split].reshape(tokens, -1)
    attended_broad = rows_first[..., split:].reshape(tokens, -1)
    projected = lax.psum_scatter(
        (
            jnp.dot(attended_narrow, project_narrow, preferred_element_type=jnp.float32)
            + jnp.dot(attended_broad, project_broad, preferred_element_type=jnp.float32)
        ).astype(jnp.bfloat16),
        "tp",
        scatter_dimension=0,
        tiled=True,
    ).astype(jnp.float32)
    mixed = (residual.astype(jnp.float32) + projected).astype(jnp.bfloat16)
    features = gather_rows(rms_scaled(mixed, norm_gain))
    tp_count, group, rows, width = features.shape
    up_total = jnp.dot(
        features.reshape(tp_count * group * rows, width),
        up_full,
        preferred_element_type=jnp.float32,
    )
    hidden = jnp.square(jax.nn.relu(up_total)).astype(jnp.bfloat16)
    down_term = jnp.dot(hidden, down_full, preferred_element_type=jnp.float32)
    parts = lax.psum_scatter(
        down_term.astype(jnp.bfloat16).reshape(features.shape),
        "tp",
        scatter_dimension=0,
        tiled=False,
    )
    summed_rows = jnp.sum(return_parts(parts).astype(jnp.float32), axis=0)
    return (mixed.astype(jnp.float32) + summed_rows).astype(jnp.bfloat16)


TICKS = (1, 2, 0, 0, 0, 1, 1, 0, 16, 0)
LOG2E = 1.4426950408889634
PIECES = 3
GATE_ROWS = 16


def split_pieces(values):
    pieces = []
    rest = values
    for _ in range(PIECES):
        piece = rest.astype(jnp.bfloat16).astype(jnp.float32)
        pieces.append(piece)
        rest = rest - piece
    return pieces


def pad_rows(values, rows):
    return jnp.concatenate(
        [values, jnp.zeros((rows - values.shape[0], values.shape[1]), values.dtype)], axis=0
    )


def pad_lanes(values, lanes):
    return jnp.concatenate(
        [values, jnp.zeros((values.shape[0], lanes - values.shape[1]), values.dtype)], axis=1
    )


def fused_kernel(
    count,
    group,
    head_groups,
    ranges,
    residual_ref,
    qn_ref,
    kn_ref,
    vn_ref,
    qb_ref,
    kb_ref,
    vb_ref,
    gn_ref,
    gb_ref,
    gain_ref,
    pn_ref,
    pb_ref,
    up_ref,
    down_ref,
    out_ref,
    q_send,
    kv_send,
    gate_send,
    q_all,
    q_gate_all,
    kv_all,
    gate_all,
    key_gates,
    v_turned,
    q_wide,
    acc,
    peaks,
    totals,
    attended,
    attended_in,
    project,
    mixed,
    normed,
    up_all,
    down_all,
    features,
    hidden,
    part_out,
    part_in,
    return_out,
    return_in,
    kv_line,
    gate_line,
    kv_plane,
    gate_plane,
    q_sems,
    q_gate_sems,
    back_sems,
    project_own,
    project_sems,
    share_sems,
    twin_sems,
    own_sems,
    across_sems,
    beside_sems,
    part_sems,
    return_sems,
):
    me = lax.axis_index("sp")
    tp = lax.axis_index("tp")
    other = 1 - tp
    planes = head_groups
    parts = count // planes
    plane = me // parts
    lane = me % parts
    base = (me // group) * group
    local = me - base
    tokens, _ = qn_ref.shape
    rows, width = residual_ref.shape
    heads = len(ranges)
    head_width = q_send.shape[2]
    narrow_width = ranges[-1][0]
    broad_width = head_width - narrow_width
    span = 2 * tokens
    barrier = pltpu.get_barrier_semaphore()

    def remote(source, target, send, recv, sp, core):
        return pltpu.make_async_remote_copy(
            src_ref=source,
            dst_ref=target,
            send_sem=send,
            recv_sem=recv,
            device_id={"sp": sp, "tp": core},
            device_id_type=pl.DeviceIdType.MESH,
        )

    def flip(place, bit):
        return place + bit * (1 - 2 * ((place // bit) % 2))

    def mate(place, offset):
        bit = 1
        while bit <= offset:
            if offset & bit:
                place = flip(place, bit)
            bit *= 2
        return place

    def hello(k, carry):
        flat = (me * 2 + tp + k) % (count * 2)
        pl.semaphore_signal(
            barrier,
            inc=1,
            device_id={"sp": flat // 2, "tp": flat % 2},
            device_id_type=pl.DeviceIdType.MESH,
        )
        return carry

    lax.fori_loop(1, count * 2, hello, 0)

    def by_group(narrow_ref, broad_ref, h):
        return [
            narrow_ref[:, h * narrow_width : (h + 1) * narrow_width],
            broad_ref[:, h * broad_width : (h + 1) * broad_width],
        ]

    narrow_heads = heads - 1
    gates = jnp.concatenate([gn_ref[...], gb_ref[...]], axis=0)
    for h in range(head_groups):
        kv_send[h] = jnp.concatenate(
            by_group(kn_ref, kb_ref, h) + by_group(vn_ref, vb_ref, h), axis=1
        )
        q_send[h] = jnp.concatenate(by_group(qn_ref, qb_ref, h), axis=1)
        lines = []
        for i, (_, _, size) in enumerate(ranges):
            if i < narrow_heads:
                source = h * narrow_heads + i
            else:
                source = head_groups * narrow_heads + h
            lines += split_pieces(gates[source : source + 1] * size**0.5)
        lines += [jnp.ones((PIECES, tokens), jnp.float32)]
        gate_send[h] = pad_rows(jnp.concatenate(lines, axis=0), GATE_ROWS).astype(jnp.bfloat16)

    pl.semaphore_wait(barrier, count * 2 - 1)

    def line_copies(j, owner):
        target = (plane + j) % planes
        peer = target * parts + lane
        return (
            remote(
                kv_send.at[target], kv_all.at[owner], kv_line.at[0, j], kv_line.at[1, j], peer, tp
            ),
            remote(
                gate_send.at[target],
                gate_all.at[owner],
                gate_line.at[0, j],
                gate_line.at[1, j],
                peer,
                tp,
            ),
        )

    def line_owner(j):
        return ((plane + planes - j) % planes) * parts + lane

    def plane_copies(j, k, kv_source, gate_source, owner):
        peer = plane * parts + mate(lane, k)
        return (
            remote(
                kv_source,
                kv_all.at[owner],
                kv_plane.at[0, j, k],
                kv_plane.at[1, j, k],
                peer,
                tp,
            ),
            remote(
                gate_source,
                gate_all.at[owner],
                gate_plane.at[0, j, k],
                gate_plane.at[1, j, k],
                peer,
                tp,
            ),
        )

    for j in range(1, planes):
        for copy in line_copies(j, me):
            copy.start()
    for k in range(1, parts):
        for copy in plane_copies(0, k, kv_send.at[plane], gate_send.at[plane], me):
            copy.start()
    kv_all[me] = kv_send[plane]
    gate_all[me] = gate_send[plane]

    double = me // 2
    reader_part = jnp.where(double < parts, double, 2 * parts - 1 - double)
    my_slot = 2 * (double // parts) + me % 2

    def query_copies(h, slot, peer):
        return (
            remote(q_send.at[h], q_all.at[slot], q_sems.at[0, h], q_sems.at[1, slot], peer, tp),
            remote(
                gate_send.at[h],
                q_gate_all.at[slot],
                q_gate_sems.at[0, h],
                q_gate_sems.at[1, slot],
                peer,
                tp,
            ),
        )

    def tile_double(tile):
        return tile * (2 * parts - 1 - lane) + (1 - tile) * lane

    for h in range(head_groups):
        reader = h * parts + reader_part

        @pl.when(reader != me)
        def _():
            for copy in query_copies(h, my_slot, reader):
                copy.start()

        @pl.when(reader == me)
        def _():
            q_all[my_slot] = q_send[h]
            q_gate_all[my_slot] = gate_send[h]

    def project_pairs(h):
        pairs = []
        for source, low, size in (
            (pn_ref, 0, narrow_width),
            (pb_ref, narrow_width, broad_width),
        ):
            pairs.append(
                (
                    source.at[h * size : (h + 1) * size, :],
                    project.at[tp * head_groups + h, low : low + size, :],
                )
            )
        return pairs

    def project_copies(h):
        own, away = [], []
        for i, (source, target) in enumerate(project_pairs(h)):
            own.append(pltpu.make_async_copy(source, target, project_own.at[h, i]))
            away.append(
                remote(
                    source,
                    target,
                    project_sems.at[0, h, i],
                    project_sems.at[1, h, i],
                    me,
                    other,
                )
            )
        return own, away

    for h in range(head_groups):
        own, away = project_copies(h)
        for copy in own + away:
            copy.start()

    units = up_all.shape[2]

    def up_source(chunk):
        return up_ref.at[:, pl.ds(pl.multiple_of(chunk * units, 128), units)]

    def down_source(chunk):
        return down_ref.at[pl.ds(pl.multiple_of(chunk * units, units), units), :]

    def share_copy(which, offset, owner):
        peer = mate(local, offset)
        source = up_source(peer) if which == 0 else down_source(peer)
        target = up_all.at[owner] if which == 0 else down_all.at[owner]
        return remote(
            source,
            target,
            share_sems.at[0, which, offset],
            share_sems.at[1, which, offset],
            base + peer,
            tp,
        )

    twin = (me + group) % count
    twin_base = (base + group) % count

    def twin_copy(which, offset, index=None):
        index = offset if index is None else index
        owner = base + mate(local, offset)
        weights = up_all if which == 0 else down_all
        if offset:
            source = weights.at[owner]
        else:
            source = up_source(local) if which == 0 else down_source(local)
        return remote(
            source,
            weights.at[owner],
            twin_sems.at[0, which, index],
            twin_sems.at[1, which, index],
            twin,
            tp,
        )

    far = group // 2
    near = [offset for offset in range(1, group) if offset != far]
    near.sort(key=(1, 6, 5, 2, 3, 7).index)
    pieces = [(0, 0), (0, far), (1, 0)] + [(0, offset) for offset in near]
    pieces += [(1, offset) for offset in (1, 2, 3, 4, 6, 5, 7)]
    issued = []

    def tick(amount):
        for _ in range(amount):
            if len(issued) == len(pieces):
                return
            which, offset = pieces[len(issued)]
            if offset:
                share_copy(which, offset, base + mate(local, offset)).wait_recv()
            twin_copy(which, offset).start()
            issued.append((which, offset))

    own_weights = [
        pltpu.make_async_copy(up_source(local), up_all.at[me], own_sems.at[0]),
        pltpu.make_async_copy(down_source(local), down_all.at[me], own_sems.at[1]),
    ]
    for copy in own_weights:
        copy.start()
    for which in range(2):
        share_copy(which, far, me).start()
    tick(TICKS[0])

    for j in range(1, planes):
        owner = line_owner(j)
        for copy in line_copies(j, owner):
            copy.wait_recv()
        for k in range(1, parts):
            for copy in plane_copies(j, k, kv_all.at[owner], gate_all.at[owner], owner):
                copy.start()

    for offset in near:
        share_copy(0, offset, me).start()
    for offset in (1, 2, 3, 6, 5, 7):
        share_copy(1, offset, me).start()
    tick(TICKS[1])

    for slot in range(4):
        owner = 2 * tile_double(slot // 2) + slot % 2

        @pl.when(owner != me)
        def _():
            for copy in query_copies(0, slot, owner):
                copy.wait_recv()

    lane_id = lax.broadcasted_iota(jnp.int32, (span, head_width), 1)
    first_one = heads * PIECES

    def turned_gates(lines):
        block = pad_lanes(pad_rows(lines.astype(jnp.float32), 128), -(-tokens // 128) * 128)
        return block.T[:tokens]

    def widen(tile, carry):
        query = q_all[pl.ds(2 * tile, 2)].reshape(span, head_width).astype(jnp.float32)
        own_gates = jnp.concatenate(
            [turned_gates(q_gate_all[2 * tile + i]) for i in range(2)], axis=0
        )
        for i, (low, high, _) in enumerate(ranges):
            left = jnp.where((lane_id >= low) & (lane_id < high), query, 0.0)
            moved = pltpu.roll(own_gates, first_one - i * PIECES, 1)
            right = jnp.where((lane_id >= first_one) & (lane_id < first_one + PIECES), moved, 0.0)
            right = jnp.where(
                (lane_id >= i * PIECES) & (lane_id < (i + 1) * PIECES), -1.0, right
            )
            q_wide[tile, i] = jnp.concatenate([left, right], axis=1).astype(jnp.bfloat16)
        acc[tile] = jnp.zeros((head_width, span), jnp.float32)
        peaks[tile] = jnp.full((heads, 1, span), -1e30, jnp.float32)
        totals[tile] = jnp.zeros((heads, 1, span), jnp.float32)
        return carry

    lax.fori_loop(0, 2, widen, 0)

    def turn(pair):
        values = kv_all[pl.ds(2 * pair, 2), :, head_width:].reshape(span, head_width)
        v_turned[pair] = values.astype(jnp.float32).T.astype(jnp.bfloat16)
        for i in range(2):
            key_gates[2 * pair + i] = turned_gates(gate_all[2 * pair + i]).astype(jnp.bfloat16)

    def attend(tile, pair, masked):
        keys = jnp.concatenate(
            [
                kv_all[pl.ds(2 * pair, 2), :, :head_width].reshape(span, head_width),
                key_gates[pl.ds(2 * pair, 2)].reshape(span, head_width),
            ],
            axis=1,
        )
        for i, (low, high, size) in enumerate(ranges):
            factor = size**-0.5 * LOG2E
            scores = lax.dot_general(
                keys, q_wide[tile, i], (((1,), (1,)), ((), ())), preferred_element_type=jnp.float32
            )
            if masked:
                row = lax.broadcasted_iota(jnp.int32, (span, span), 0)
                column = lax.broadcasted_iota(jnp.int32, (span, span), 1)
                scores = jnp.where(row <= column, scores, -1e30)
            before = peaks[tile, i]
            peak = jnp.maximum(before, jnp.max(scores, axis=0, keepdims=True))
            weights = jnp.exp2((scores - peak) * factor)
            fade = jnp.exp2((before - peak) * factor)
            peaks[tile, i] = peak
            totals[tile, i] = totals[tile, i] * fade + jnp.sum(weights, axis=0, keepdims=True)
            acc[tile, low:high, :] = acc[tile, low:high, :] * fade + jnp.dot(
                v_turned[pair, low:high, :],
                weights.astype(jnp.bfloat16),
                preferred_element_type=jnp.float32,
            )

    for j in range(planes):
        source_plane = (plane + planes - j) % planes
        for k in range(1, parts):
            owner = source_plane * parts + mate(lane, k)
            for copy in plane_copies(j, k, kv_all.at[owner], gate_all.at[owner], owner):
                copy.wait_recv()

        def visit(i, carry):
            pair = source_plane * (parts // 2) + i // 2
            tile = i % 2
            double_block = tile_double(tile)

            @pl.when(tile == 0)
            def _():
                turn(pair)

            @pl.when(pair < double_block)
            def _():
                attend(tile, pair, False)

            @pl.when(pair == double_block)
            def _():
                attend(tile, pair, True)

            return carry

        lax.fori_loop(0, parts, visit, 0)
        tick(TICKS[2 + j])

    def settle(tile, carry):
        scaled = jnp.concatenate(
            [acc[tile, low:high, :] / totals[tile, i] for i, (low, high, _) in enumerate(ranges)],
            axis=0,
        )
        attended[pl.ds(2 * tile, 2)] = (
            scaled.T.astype(jnp.bfloat16).reshape(2, tokens, head_width)
        )
        return carry

    lax.fori_loop(0, 2, settle, 0)

    def back_copy(slot, core, place, sp):
        return remote(
            attended.at[slot, core * rows : (core + 1) * rows, :],
            attended_in.at[place],
            back_sems.at[0, slot, core],
            back_sems.at[1, 0, place],
            sp,
            core,
        )

    my_place = tp * head_groups + plane
    for slot in range(4):
        owner = 2 * tile_double(slot // 2) + slot % 2
        for core in range(2):
            here = (owner == me) & (tp == core)

            @pl.when(jnp.logical_not(here))
            def _():
                back_copy(slot, core, my_place, owner).start()

            @pl.when(here)
            def _():
                attended_in[my_place] = attended[slot, core * rows : (core + 1) * rows, :]

    tick(TICKS[6])
    for h in range(head_groups):
        own, away = project_copies(h)
        for copy in own:
            copy.wait()
        for copy in away:
            copy.wait()
    for h in range(head_groups):
        for core in range(2):
            place = core * head_groups + h
            sender = h * parts + reader_part

            @pl.when(jnp.logical_not((sender == me) & (tp == core)))
            def _():
                remote(
                    attended.at[0, :rows, :],
                    attended_in.at[place],
                    back_sems.at[0, 0, 0],
                    back_sems.at[1, 0, place],
                    sender,
                    core,
                ).wait_recv()

    step_width = return_out.shape[3]
    chunks = width // step_width
    joined = jnp.concatenate([attended_in[i] for i in range(2 * head_groups)], axis=1)

    def project_step(n, squares):
        columns = pl.ds(pl.multiple_of(n * step_width, step_width), step_width)
        total = residual_ref[:, columns].astype(jnp.float32) + jnp.dot(
            joined,
            project[:, :, columns].reshape(2 * head_groups * head_width, step_width),
            preferred_element_type=jnp.float32,
        )
        total = total.astype(jnp.bfloat16).astype(jnp.float32)
        mixed[:, columns] = total
        return squares + jnp.sum(total * total, axis=1, keepdims=True)

    tick(TICKS[7])
    squares = lax.fori_loop(0, chunks, project_step, jnp.zeros((rows, 1), jnp.float32))
    scale = lax.rsqrt(squares / width + 1e-06)
    scaled_rows = (mixed[...] * scale * gain_ref[...]).astype(jnp.bfloat16)
    normed[...] = scaled_rows
    features[tp, local] = scaled_rows

    bits = (group // 2, 1 + tp, 2 - tp)
    levels = len(bits)

    def member(subset):
        place = local
        for level in range(levels):
            if (subset >> level) & 1:
                place = flip(place, bits[level])
        return place

    def across(subset):
        level = subset.bit_length() - 1
        held = subset - (1 << level)
        owner = member(held)
        return remote(
            features.at[tp, owner] if held else normed,
            features.at[tp, owner],
            across_sems.at[0, subset],
            across_sems.at[1, subset],
            base + flip(local, bits[level]),
            tp,
        )

    def beside(subset):
        owner = member(subset)
        return remote(
            features.at[tp, owner] if subset else normed,
            features.at[tp, owner],
            beside_sems.at[0, subset],
            beside_sems.at[1, subset],
            me,
            other,
        )

    def spread(subset):
        for level in range(subset.bit_length(), levels):
            across(subset + (1 << level)).start()
        beside(subset).start()

    spread(0)
    tick(TICKS[8])
    for subset in (2, 1, 3):
        across(subset).wait_recv()
        spread(subset)
        tick(TICKS[9])
    tick(len(pieces))
    own_weights[0].wait()
    row_groups = 2
    some = group // row_groups

    def up_step(core, place):
        chips = pl.ds(place * some, some)
        total = jnp.dot(
            features[core, chips].reshape(some * rows, width),
            up_all[...].reshape(width, units),
            preferred_element_type=jnp.float32,
        )
        total = jnp.maximum(total, 0.0)
        hidden[core, chips] = (
            (total * total).astype(jnp.bfloat16).reshape(some, rows, units)
        )

    home = local // some
    for subset in (4, 6):
        across(subset).wait_recv()
        spread(subset)
    for subset in (0, 2, 4, 6):
        beside(subset).wait_recv()
    for offset in range(group):
        twin_copy(0, offset).wait_recv()

    def up_both(place):
        def inner(core, carry):
            up_step(core, place)
            return carry

        lax.fori_loop(0, 2, inner, 0)

    up_both(home)
    for subset in (5, 7):
        across(subset).wait_recv()
        spread(subset)
    for subset in (1, 3, 5, 7):
        beside(subset).wait_recv()
    up_both(1 - home)
    own_weights[1].wait()
    per_chunk = count // chunks

    def chunk_of(i):
        return ((base + (i // 2) * group) % count) // per_chunk + (local // per_chunk + i) % 2

    def wait_down(i):
        if i >= chunks // 2:
            for k in range(per_chunk):
                twin_copy(1, (i % 2) * per_chunk + k).wait_recv()

    def down_columns(chunk):
        return jnp.concatenate(
            [down_all[chunk * per_chunk + i] for i in range(per_chunk)], axis=1
        )

    def part_copy(chunk):
        return remote(
            part_out.at[chunk],
            part_in.at[chunk],
            part_sems.at[0, chunk],
            part_sems.at[1, chunk],
            me,
            other,
        )

    def down_dot(core, chips, chunk):
        return jnp.dot(
            hidden[core, chips].reshape(some * rows, units),
            down_columns(chunk),
            preferred_element_type=jnp.float32,
        ).reshape(some, rows, step_width)

    def away_step(chunk):
        def inner(i, carry):
            chips = pl.ds(i * some, some)
            part_out[chunk, chips] = down_dot(other, chips, chunk).astype(jnp.bfloat16)
            return carry

        lax.fori_loop(0, row_groups, inner, 0)
        part_copy(chunk).start()


    def return_copy(chunk, subset):
        level = subset.bit_length() - 1
        return remote(
            return_out.at[chunk, member(subset)],
            return_in.at[chunk, subset],
            return_sems.at[0, chunk, subset],
            return_sems.at[1, chunk, subset],
            base + flip(local, bits[level]),
            tp,
        )

    def home_step(chunk):
        part_copy(chunk).wait_recv()

        def inner(i, carry):
            chips = pl.ds(i * some, some)
            return_out[chunk, chips] = (
                down_dot(tp, chips, chunk) + part_in[chunk, chips].astype(jnp.float32)
            ).astype(jnp.bfloat16)
            return carry

        lax.fori_loop(0, row_groups, inner, 0)
        for subset in range(group // 2, group):
            return_copy(chunk, subset).start()

    wait_down(0)
    away_step(chunk_of(0))
    for i in range(chunks):
        if i + 1 < chunks:
            wait_down(i + 1)
            away_step(chunk_of(i + 1))
        home_step(chunk_of(i))

    for level in range(levels - 1, 0, -1):

        def merge_step(i, carry):
            chunk = chunk_of(i)
            for held in range(1 << level):
                return_copy(chunk, held + (1 << level)).wait_recv()
                place = member(held)
                return_out[chunk, place] = (
                    return_out[chunk, place].astype(jnp.float32)
                    + return_in[chunk, held + (1 << level)].astype(jnp.float32)
                ).astype(jnp.bfloat16)
            for subset in range(1 << (level - 1), 1 << level):
                return_copy(chunk, subset).start()
            return carry

        lax.fori_loop(0, chunks, merge_step, 0)

    def final_step(i, carry):
        chunk = chunk_of(i)
        columns = pl.ds(pl.multiple_of(chunk * step_width, step_width), step_width)
        return_copy(chunk, 1).wait_recv()
        total = (
            mixed[:, columns]
            + return_out[chunk, local].astype(jnp.float32)
            + return_in[chunk, 1].astype(jnp.float32)
        )
        out_ref[:, columns] = total.astype(jnp.bfloat16)
        return carry

    lax.fori_loop(0, chunks, final_step, 0)

    for j in range(1, planes):
        for copy in line_copies(j, me):
            copy.wait_send()
    for j in range(planes):
        for k in range(1, parts):
            for copy in plane_copies(j, k, kv_send.at[plane], gate_send.at[plane], me):
                copy.wait_send()
    for h in range(head_groups):
        reader = h * parts + reader_part

        @pl.when(reader != me)
        def _():
            for copy in query_copies(h, my_slot, reader):
                copy.wait_send()

    for slot in range(4):
        owner = 2 * tile_double(slot // 2) + slot % 2
        for core in range(2):
            here = (owner == me) & (tp == core)

            @pl.when(jnp.logical_not(here))
            def _():
                back_copy(slot, core, my_place, owner).wait_send()

    for which in range(2):
        for offset in range(1, group):
            share_copy(which, offset, me).wait_send()
    for which, offset in pieces:
        twin_copy(which, offset).wait_send()
    for subset in range(group):
        if subset:
            across(subset).wait_send()
        beside(subset).wait_send()

    def returns_sent(chunk, carry):
        part_copy(chunk).wait_send()
        for subset in range(1, group):
            return_copy(chunk, subset).wait_send()
        return carry

    lax.fori_loop(0, chunks, returns_sent, 0)


def fused_local(
    residual,
    queries_narrow,
    keys_narrow,
    values_narrow,
    queries_broad,
    keys_broad,
    values_broad,
    gates_narrow,
    gates_broad,
    project_narrow,
    project_broad,
    norm_gain,
    up_weight,
    down_weight,
):
    count = lax.axis_size("sp")
    group = group_size(count)
    tokens = queries_narrow.shape[0]
    rows, width = residual.shape
    head_groups = gates_broad.shape[1]
    parts = count // head_groups
    narrow_heads = gates_narrow.shape[1] // head_groups
    ranges = head_columns(narrow_heads)
    heads = len(ranges)
    head_width = ranges[-1][1]
    up_rows, unit_total = up_weight.shape
    units = unit_total // group
    columns = down_weight.shape[1]
    step_width = 4 * columns
    chunks = width // step_width
    span = 2 * tokens
    kind = residual.dtype
    vmem = pl.BlockSpec(memory_space=pltpu.VMEM)
    anywhere = pl.BlockSpec(memory_space=pl.ANY)
    dma = pltpu.SemaphoreType.DMA
    returned = (chunks, group, rows, step_width)
    return pl.pallas_call(
        functools.partial(fused_kernel, count, group, head_groups, ranges),
        out_shape=jax.ShapeDtypeStruct(residual.shape, kind),
        in_specs=[vmem] * 10 + [anywhere] * 4,
        out_specs=vmem,
        scratch_shapes=[
            pltpu.VMEM((head_groups, tokens, head_width), kind),
            pltpu.VMEM((head_groups, tokens, 2 * head_width), kind),
            pltpu.VMEM((head_groups, GATE_ROWS, tokens), kind),
            pltpu.VMEM((4, tokens, head_width), kind),
            pltpu.VMEM((4, GATE_ROWS, tokens), kind),
            pltpu.VMEM((count, tokens, 2 * head_width), kind),
            pltpu.VMEM((count, GATE_ROWS, tokens), kind),
            pltpu.VMEM((count, tokens, head_width), kind),
            pltpu.VMEM((count // 2, head_width, span), kind),
            pltpu.VMEM((2, heads, span, 2 * head_width), kind),
            pltpu.VMEM((2, head_width, span), jnp.float32),
            pltpu.VMEM((2, heads, 1, span), jnp.float32),
            pltpu.VMEM((2, heads, 1, span), jnp.float32),
            pltpu.VMEM((4, tokens, head_width), kind),
            pltpu.VMEM((2 * head_groups, rows, head_width), kind),
            pltpu.VMEM((2 * head_groups, head_width, width), kind),
            pltpu.VMEM((rows, width), jnp.float32),
            pltpu.VMEM((rows, width), kind),
            pltpu.VMEM((count, up_rows, units), kind),
            pltpu.VMEM((count, units, columns), kind),
            pltpu.VMEM((2, group, rows, width), kind),
            pltpu.VMEM((2, group, rows, units), kind),
            pltpu.VMEM(returned, kind),
            pltpu.VMEM(returned, kind),
            pltpu.VMEM(returned, kind),
            pltpu.VMEM(returned, kind),
            dma((2, head_groups)),
            dma((2, head_groups)),
            dma((2, head_groups, parts)),
            dma((2, head_groups, parts)),
            dma((2, 4)),
            dma((2, 4)),
            dma((2, 4, 2 * head_groups)),
            dma((head_groups, 2)),
            dma((2, head_groups, 2)),
            dma((2, 2, group)),
            dma((2, 2, group)),
            dma((2,)),
            dma((2, group)),
            dma((2, group)),
            dma((2, chunks)),
            dma((2, chunks, group)),
        ],
        compiler_params=pltpu.CompilerParams(
            collective_id=3, has_side_effects=True, vmem_limit_bytes=60 * 2**20
        ),
    )(
        residual,
        queries_narrow,
        keys_narrow,
        values_narrow,
        queries_broad,
        keys_broad,
        values_broad,
        gates_narrow.T,
        gates_broad.T,
        norm_gain.reshape(1, -1),
        project_narrow,
        project_broad,
        up_weight,
        down_weight,
    )


def layer(*arrays):
    queries, gates_broad, down_weight = arrays[1], arrays[8], arrays[13]
    head_groups = gates_broad.shape[1]
    narrow_heads = arrays[7].shape[1] // head_groups
    fused = (
        lax.axis_size("tp") == 2
        and head_groups == 4
        and lax.axis_size("sp") == head_groups * 4
        and group_size(lax.axis_size("sp")) == 8
        and narrow_heads * A_DIM + B_DIM == 128
        and down_weight.shape[1] % 128 == 0
        and queries.shape[0] % 64 == 0
    )
    return fused_local(*arrays) if fused else local(*arrays)


def solution(mesh):
    return jax.shard_map(
        layer,
        mesh=mesh,
        in_specs=(
            P(("sp", "tp"), None),
            P("sp", "tp"),
            P("sp", "tp"),
            P("sp", "tp"),
            P("sp", "tp"),
            P("sp", "tp"),
            P("sp", "tp"),
            P("sp", "tp"),
            P("sp", "tp"),
            P("tp", None),
            P("tp", None),
            P(),
            P("sp", "tp"),
            P("tp", "sp"),
        ),
        out_specs=P(("sp", "tp"), None),
        check_vma=False,
    )
```

```python
import functools

import jax
import jax.numpy as jnp
from jax import lax
from jax.experimental import pallas as pl
from jax.experimental.pallas import tpu as pltpu
from jax.sharding import PartitionSpec as P

A_DIM = 32
B_DIM = 64


def rms_scaled(mixed, norm_gain):
    mixed_wide = mixed.astype(jnp.float32)
    scale = lax.rsqrt(jnp.mean(mixed_wide * mixed_wide, axis=-1, keepdims=True) + 1e-06)
    return (mixed_wide * scale * norm_gain).astype(jnp.bfloat16)


def group_size(sp_count):
    return 8 if sp_count % 8 == 0 else sp_count


def head_columns(narrow_heads):
    ranges = [(h * A_DIM, (h + 1) * A_DIM, A_DIM) for h in range(narrow_heads)]
    return ranges + [(narrow_heads * A_DIM, narrow_heads * A_DIM + B_DIM, B_DIM)]


def attend_block(ranges, block, query, kv_all, gate_all):
    tokens, width = query.shape
    lane = lax.broadcasted_iota(jnp.int32, (tokens, width), 1)
    row = lax.broadcasted_iota(jnp.int32, (tokens, tokens), 0)
    column = lax.broadcasted_iota(jnp.int32, (tokens, tokens), 1)
    inside = [(lane >= low) & (lane < high) for low, high, _ in ranges]
    wide = query.astype(jnp.float32)
    head_queries = [jnp.where(mask, wide, 0.0).astype(jnp.bfloat16) for mask in inside]
    own_gates = gate_all[block]
    query_gates = [
        jnp.sum(jnp.where(row == column, own_gates[h : h + 1, :], 0.0), axis=1, keepdims=True)
        for h in range(len(ranges))
    ]

    def by_head(columns):
        spread = jnp.broadcast_to(columns[-1], (tokens, width))
        for mask, values in zip(inside[:-1], columns[:-1]):
            spread = jnp.where(mask, values, spread)
        return spread

    def step(key_block, state):
        peaks, totals, summed = state
        keys = kv_all[key_block, :, :width]
        values = kv_all[key_block, :, width:]
        key_gates = gate_all[key_block]
        allowed = column + (key_block - block) * tokens <= row
        new_peaks, new_totals, fades, terms = [], [], [], []
        for h, (_, _, size) in enumerate(ranges):
            scores = (
                lax.dot_general(
                    head_queries[h],
                    keys,
                    (((1,), (1,)), ((), ())),
                    preferred_element_type=jnp.float32,
                )
                * size ** (-0.5)
                + query_gates[h]
                - key_gates[h : h + 1, :]
            )
            scores = jnp.where(allowed, scores, -1e30)
            peak = jnp.maximum(peaks[h], jnp.max(scores, axis=1, keepdims=True))
            weights = jnp.exp(scores - peak)
            fade = jnp.exp(peaks[h] - peak)
            new_peaks.append(peak)
            new_totals.append(totals[h] * fade + jnp.sum(weights, axis=1, keepdims=True))
            fades.append(fade)
            terms.append(
                jnp.dot(
                    weights.astype(jnp.bfloat16), values, preferred_element_type=jnp.float32
                )
            )
        summed = summed * by_head(fades) + by_head(terms)
        return tuple(new_peaks), tuple(new_totals), summed

    heads = len(ranges)
    initial = (
        tuple(jnp.full((tokens, 1), -1e30, jnp.float32) for _ in range(heads)),
        tuple(jnp.zeros((tokens, 1), jnp.float32) for _ in range(heads)),
        jnp.zeros((tokens, width), jnp.float32),
    )
    _, totals, summed = lax.fori_loop(0, block + 1, step, initial)
    return (summed / by_head(totals)).astype(jnp.bfloat16)


def layer_kernel(
    count,
    group,
    ranges,
    q_ref,
    kv_ref,
    gate_ref,
    up_ref,
    down_ref,
    attended_out,
    up_out,
    down_out,
    q_all,
    kv_all,
    gate_all,
    attended,
    up_hold,
    down_hold,
    kv_sems,
    gate_sems,
    q_sems,
    back_sems,
    sems,
    own_sems,
):
    me = lax.axis_index("sp")
    head_groups = q_ref.shape[0]
    parts = count // head_groups
    my_heads = me % head_groups
    my_part = me // head_groups

    def block_of(part, slot):
        turn = slot % 2
        return slot * parts + (1 - turn) * part + turn * (parts - 1 - part)

    my_slot = me // parts
    my_turn = my_slot % 2
    place = me % parts
    reader_part = (1 - my_turn) * place + my_turn * (parts - 1 - place)
    up_rows = up_ref.shape[0]
    units = up_out.shape[1]
    columns = down_ref.shape[1]
    barrier = pltpu.get_barrier_semaphore()

    def hello(k, carry):
        pl.semaphore_signal(
            barrier,
            inc=1,
            device_id={"sp": (me + k) % count},
            device_id_type=pl.DeviceIdType.MESH,
        )
        return carry

    lax.fori_loop(1, count, hello, 0)
    pl.semaphore_wait(barrier, count - 1)

    def remote(source, target, sem_pair, first, second, peer):
        return pltpu.make_async_remote_copy(
            src_ref=source,
            dst_ref=target,
            send_sem=sem_pair.at[0, first],
            recv_sem=sem_pair.at[1, second],
            device_id={"sp": peer},
            device_id_type=pl.DeviceIdType.MESH,
        )

    def context_copies(k, owner):
        peer = (me + k) % count
        heads = peer % head_groups
        return (
            remote(kv_ref.at[heads], kv_all.at[owner], kv_sems, k, k, peer),
            remote(gate_ref.at[heads], gate_all.at[owner], gate_sems, k, k, peer),
        )

    def start_context(k, carry):
        for copy in context_copies(k, me):
            copy.start()
        return carry

    def wait_context(k, carry):
        for copy in context_copies(k, (me + count - k) % count):
            copy.wait_recv()
            copy.wait_send()
        return carry

    for heads in range(head_groups):
        reader = reader_part * head_groups + heads

        @pl.when(reader != me)
        def _():
            remote(q_ref.at[heads], q_all.at[my_slot], q_sems, heads, my_slot, reader).start()

        @pl.when(reader == me)
        def _():
            q_all[my_slot] = q_ref[heads]

    lax.fori_loop(1, count, start_context, 0)
    kv_all[me] = kv_ref[my_heads]
    gate_all[me] = gate_ref[my_heads]

    def up_source(chunk):
        return up_ref.at[:, pl.ds(pl.multiple_of(chunk * units, 128), units)]

    def down_source(chunk):
        return down_ref.at[pl.ds(pl.multiple_of(chunk * units, units), units), :]

    def up_target(owner):
        return up_out.at[pl.ds(pl.multiple_of(owner * up_rows, up_rows), up_rows), :]

    def down_target(owner):
        if len(down_out.shape) == 3:
            return down_out.at[owner]
        return down_out.at[:, pl.ds(pl.multiple_of(owner * columns, columns), columns)]

    def copies(k, target_owner):
        peer = (me + k) % count
        chunk = peer % group
        pairs = (
            (up_source(chunk), up_target(target_owner)),
            (down_source(chunk), down_target(target_owner)),
        )
        return [
            pltpu.make_async_remote_copy(
                src_ref=source,
                dst_ref=target,
                send_sem=sems.at[0, which, k],
                recv_sem=sems.at[1, which, k],
                device_id={"sp": peer},
                device_id_type=pl.DeviceIdType.MESH,
            )
            for which, (source, target) in enumerate(pairs)
        ]

    def start(k, carry):
        for copy in copies(k, me):
            copy.start()
        return carry

    def finish(k, carry):
        for copy in copies(k, (me + count - k) % count):
            copy.wait_recv()
            copy.wait_send()
        return carry

    lax.fori_loop(1, count, start, 0)
    own = me % group
    first = [
        pltpu.make_async_copy(up_source(own), up_hold, own_sems.at[0]),
        pltpu.make_async_copy(down_source(own), down_hold, own_sems.at[1]),
    ]
    for copy in first:
        copy.start()
    for copy in first:
        copy.wait()
    second = [
        pltpu.make_async_copy(up_hold, up_target(me), own_sems.at[0]),
        pltpu.make_async_copy(down_hold, down_target(me), own_sems.at[1]),
    ]
    for copy in second:
        copy.start()
    for heads in range(head_groups):
        reader = reader_part * head_groups + heads

        @pl.when(reader != me)
        def _():
            remote(q_ref.at[heads], q_all.at[my_slot], q_sems, heads, my_slot, reader).wait_send()

    for slot in range(head_groups):
        owner = block_of(my_part, slot)

        @pl.when(owner != me)
        def _():
            remote(q_ref.at[0], q_all.at[slot], q_sems, 0, slot, owner).wait_recv()

    lax.fori_loop(1, count, wait_context, 0)

    def attend(slot, carry):
        block = block_of(my_part, slot)
        attended[slot] = attend_block(ranges, block, q_all[slot], kv_all, gate_all)
        return carry

    lax.fori_loop(0, head_groups, attend, 0)
    for slot in range(head_groups):
        owner = block_of(my_part, slot)

        @pl.when(owner != me)
        def _():
            remote(
                attended.at[slot], attended_out.at[my_heads], back_sems, slot, my_heads, owner
            ).start()

        @pl.when(owner == me)
        def _():
            attended_out[my_heads] = attended[slot]

    for copy in second:
        copy.wait()
    lax.fori_loop(1, count, finish, 0)
    for slot in range(head_groups):
        owner = block_of(my_part, slot)

        @pl.when(owner != me)
        def _():
            remote(
                attended.at[slot], attended_out.at[my_heads], back_sems, slot, my_heads, owner
            ).wait_send()

    for heads in range(head_groups):
        reader = reader_part * head_groups + heads

        @pl.when(reader != me)
        def _():
            remote(
                attended.at[0], attended_out.at[heads], back_sems, 0, heads, reader
            ).wait_recv()


def attend_and_share(queries, keys_values, gates, ranges, up_weight, down_weight):
    head_groups, tokens, head_width = queries.shape
    count = lax.axis_size("sp")
    group = group_size(count)
    up_rows, unit_total = up_weight.shape
    columns = down_weight.shape[1]
    units = unit_total // group
    if columns % 128 == 0:
        down_shape = (units, count * columns)
    else:
        down_shape = (count, units, columns)
    attended, up_full, down_full = pl.pallas_call(
        functools.partial(layer_kernel, count, group, ranges),
        out_shape=(
            jax.ShapeDtypeStruct(queries.shape, queries.dtype),
            jax.ShapeDtypeStruct((count * up_rows, units), up_weight.dtype),
            jax.ShapeDtypeStruct(down_shape, down_weight.dtype),
        ),
        in_specs=[pl.BlockSpec(memory_space=pltpu.VMEM)] * 3
        + [pl.BlockSpec(memory_space=pl.ANY)] * 2,
        out_specs=[pl.BlockSpec(memory_space=pltpu.VMEM)]
        + [pl.BlockSpec(memory_space=pl.ANY)] * 2,
        scratch_shapes=[
            pltpu.VMEM(queries.shape, queries.dtype),
            pltpu.VMEM((count,) + keys_values.shape[1:], keys_values.dtype),
            pltpu.VMEM((count,) + gates.shape[1:], gates.dtype),
            pltpu.VMEM(queries.shape, queries.dtype),
            pltpu.VMEM((up_rows, units), up_weight.dtype),
            pltpu.VMEM((units, columns), down_weight.dtype),
            pltpu.SemaphoreType.DMA((2, count)),
            pltpu.SemaphoreType.DMA((2, count)),
            pltpu.SemaphoreType.DMA((2, head_groups)),
            pltpu.SemaphoreType.DMA((2, head_groups)),
            pltpu.SemaphoreType.DMA((2, 2, count)),
            pltpu.SemaphoreType.DMA((2,)),
        ],
        compiler_params=pltpu.CompilerParams(collective_id=0, has_side_effects=True),
        cost_estimate=pl.CostEstimate(
            flops=0, bytes_accessed=count * up_rows * units * 80, transcendentals=0
        ),
    )(queries, keys_values, gates, up_weight, down_weight)
    if columns % 128:
        down_full = down_full.transpose(1, 0, 2).reshape(units, count * columns)
    return attended, up_full, down_full


def gather_kernel(group, tp_count, rows_ref, out_ref, hold, sems, own_sems, pass_sems):
    sp = lax.axis_index("sp")
    tp = lax.axis_index("tp")
    base = (sp // group) * group
    me = sp - base
    barrier = pltpu.get_barrier_semaphore()
    for k in range(1, group):
        pl.semaphore_signal(
            barrier,
            inc=1,
            device_id={"sp": base + (me + k) % group},
            device_id_type=pl.DeviceIdType.MESH,
        )
    for j in range(1, tp_count):
        pl.semaphore_signal(
            barrier,
            inc=1,
            device_id={"tp": (tp + j) % tp_count},
            device_id_type=pl.DeviceIdType.MESH,
        )
    pl.semaphore_wait(barrier, group + tp_count - 2)

    def across(k, owner):
        return pltpu.make_async_remote_copy(
            src_ref=rows_ref,
            dst_ref=out_ref.at[tp, owner],
            send_sem=sems.at[0, k],
            recv_sem=sems.at[1, k],
            device_id={"sp": base + (me + k) % group},
            device_id_type=pl.DeviceIdType.MESH,
        )

    def beside(j, k, source, tp_owner, owner):
        return pltpu.make_async_remote_copy(
            src_ref=source,
            dst_ref=out_ref.at[tp_owner, owner],
            send_sem=pass_sems.at[0, j, k],
            recv_sem=pass_sems.at[1, j, k],
            device_id={"tp": (tp + j) % tp_count},
            device_id_type=pl.DeviceIdType.MESH,
        )

    for k in range(1, group):
        across(k, me).start()
    for j in range(1, tp_count):
        beside(j, 0, rows_ref, tp, me).start()
    own = pltpu.make_async_copy(rows_ref, hold, own_sems.at[0])
    own.start()
    own.wait()
    own = pltpu.make_async_copy(hold, out_ref.at[tp, me], own_sems.at[1])
    own.start()
    own.wait()
    for k in range(1, group):
        owner = (me + group - k) % group
        across(k, owner).wait_recv()
        for j in range(1, tp_count):
            beside(j, k, out_ref.at[tp, owner], tp, owner).start()
    for k in range(1, group):
        across(k, me).wait_send()
    for j in range(1, tp_count):
        for k in range(group):
            owner = (me + group - k) % group
            copy = beside(j, k, rows_ref, (tp + tp_count - j) % tp_count, owner)
            copy.wait_send()
            copy.wait_recv()


def gather_rows(rows):
    group = group_size(lax.axis_size("sp"))
    tp_count = lax.axis_size("tp")
    return pl.pallas_call(
        functools.partial(gather_kernel, group, tp_count),
        out_shape=jax.ShapeDtypeStruct((tp_count, group) + rows.shape, rows.dtype),
        in_specs=[pl.BlockSpec(memory_space=pl.ANY)],
        out_specs=pl.BlockSpec(memory_space=pl.ANY),
        scratch_shapes=[
            pltpu.VMEM(rows.shape, rows.dtype),
            pltpu.SemaphoreType.DMA((2, group)),
            pltpu.SemaphoreType.DMA((2,)),
            pltpu.SemaphoreType.DMA((2, tp_count, group)),
        ],
        compiler_params=pltpu.CompilerParams(collective_id=1, has_side_effects=True),
    )(rows)


def return_kernel(group, parts_ref, out_ref, hold, sems, own_sems):
    sp = lax.axis_index("sp")
    base = (sp // group) * group
    me = sp - base
    barrier = pltpu.get_barrier_semaphore()
    for k in range(1, group):
        pl.semaphore_signal(
            barrier,
            inc=1,
            device_id={"sp": base + (me + k) % group},
            device_id_type=pl.DeviceIdType.MESH,
        )
    pl.semaphore_wait(barrier, group - 1)

    def across(k, owner):
        peer = (me + k) % group
        return pltpu.make_async_remote_copy(
            src_ref=parts_ref.at[peer],
            dst_ref=out_ref.at[owner],
            send_sem=sems.at[0, k],
            recv_sem=sems.at[1, k],
            device_id={"sp": base + peer},
            device_id_type=pl.DeviceIdType.MESH,
        )

    for k in range(1, group):
        across(k, me).start()
    own = pltpu.make_async_copy(parts_ref.at[me], hold, own_sems.at[0])
    own.start()
    own.wait()
    own = pltpu.make_async_copy(hold, out_ref.at[me], own_sems.at[1])
    own.start()
    own.wait()
    for k in range(1, group):
        copy = across(k, (me + group - k) % group)
        copy.wait_recv()
        copy.wait_send()


def return_parts(parts):
    group = parts.shape[0]
    return pl.pallas_call(
        functools.partial(return_kernel, group),
        out_shape=jax.ShapeDtypeStruct(parts.shape, parts.dtype),
        in_specs=[pl.BlockSpec(memory_space=pl.ANY)],
        out_specs=pl.BlockSpec(memory_space=pl.ANY),
        scratch_shapes=[
            pltpu.VMEM(parts.shape[1:], parts.dtype),
            pltpu.SemaphoreType.DMA((2, group)),
            pltpu.SemaphoreType.DMA((2,)),
        ],
        compiler_params=pltpu.CompilerParams(collective_id=2, has_side_effects=True),
    )(parts)


def local(
    residual,
    queries_narrow,
    keys_narrow,
    values_narrow,
    queries_broad,
    keys_broad,
    values_broad,
    gates_narrow,
    gates_broad,
    project_narrow,
    project_broad,
    norm_gain,
    up_weight,
    down_weight,
):
    tokens = queries_narrow.shape[0]
    head_groups = gates_broad.shape[1]
    narrow_heads = gates_narrow.shape[1] // head_groups
    ranges = head_columns(narrow_heads)

    def by_group(narrow, broad):
        return jnp.concatenate(
            [part.reshape(tokens, head_groups, -1) for part in (narrow, broad)], axis=-1
        ).transpose(1, 0, 2)

    gates = jnp.concatenate(
        [gates_narrow.reshape(tokens, head_groups, narrow_heads), gates_broad[..., None]], axis=-1
    ).transpose(1, 2, 0)
    gates = jnp.pad(gates, ((0, 0), (0, -gates.shape[1] % 8), (0, 0)))
    attended, up_full, down_full = attend_and_share(
        by_group(queries_narrow, queries_broad),
        jnp.concatenate(
            [by_group(keys_narrow, keys_broad), by_group(values_narrow, values_broad)], axis=-1
        ),
        gates,
        ranges,
        up_weight,
        down_weight,
    )
    rows_first = attended.transpose(1, 0, 2)
    split = narrow_heads * A_DIM
    attended_narrow = rows_first[..., :split].reshape(tokens, -1)
    attended_broad = rows_first[..., split:].reshape(tokens, -1)
    projected = lax.psum_scatter(
        (
            jnp.dot(attended_narrow, project_narrow, preferred_element_type=jnp.float32)
            + jnp.dot(attended_broad, project_broad, preferred_element_type=jnp.float32)
        ).astype(jnp.bfloat16),
        "tp",
        scatter_dimension=0,
        tiled=True,
    ).astype(jnp.float32)
    mixed = (residual.astype(jnp.float32) + projected).astype(jnp.bfloat16)
    features = gather_rows(rms_scaled(mixed, norm_gain))
    tp_count, group, rows, width = features.shape
    up_total = jnp.dot(
        features.reshape(tp_count * group * rows, width),
        up_full,
        preferred_element_type=jnp.float32,
    )
    hidden = jnp.square(jax.nn.relu(up_total)).astype(jnp.bfloat16)
    down_term = jnp.dot(hidden, down_full, preferred_element_type=jnp.float32)
    parts = lax.psum_scatter(
        down_term.astype(jnp.bfloat16).reshape(features.shape),
        "tp",
        scatter_dimension=0,
        tiled=False,
    )
    summed_rows = jnp.sum(return_parts(parts).astype(jnp.float32), axis=0)
    return (mixed.astype(jnp.float32) + summed_rows).astype(jnp.bfloat16)


TICKS = (1, 3, 0, 0, 0, 1, 2, 0, 16, 0)
LOG2E = 1.4426950408889634
PIECES = 3
GATE_ROWS = 16


def split_pieces(values):
    pieces = []
    rest = values
    for _ in range(PIECES):
        piece = rest.astype(jnp.bfloat16).astype(jnp.float32)
        pieces.append(piece)
        rest = rest - piece
    return pieces


def pad_rows(values, rows):
    return jnp.concatenate(
        [values, jnp.zeros((rows - values.shape[0], values.shape[1]), values.dtype)], axis=0
    )


def pad_lanes(values, lanes):
    return jnp.concatenate(
        [values, jnp.zeros((values.shape[0], lanes - values.shape[1]), values.dtype)], axis=1
    )


def fused_kernel(
    count,
    group,
    head_groups,
    ranges,
    residual_ref,
    qn_ref,
    kn_ref,
    vn_ref,
    qb_ref,
    kb_ref,
    vb_ref,
    gn_ref,
    gb_ref,
    gain_ref,
    pn_ref,
    pb_ref,
    up_ref,
    down_ref,
    out_ref,
    q_send,
    kv_send,
    gate_send,
    q_all,
    q_gate_all,
    kv_all,
    gate_all,
    key_gates,
    v_turned,
    q_wide,
    acc,
    peaks,
    totals,
    attended,
    attended_in,
    project,
    mixed,
    normed,
    up_all,
    down_all,
    features,
    hidden,
    part_out,
    part_in,
    return_out,
    return_in,
    kv_line,
    gate_line,
    kv_plane,
    gate_plane,
    q_sems,
    q_gate_sems,
    back_sems,
    project_own,
    project_sems,
    share_sems,
    twin_sems,
    own_sems,
    across_sems,
    beside_sems,
    part_sems,
    return_sems,
):
    me = lax.axis_index("sp")
    tp = lax.axis_index("tp")
    other = 1 - tp
    planes = head_groups
    parts = count // planes
    plane = me // parts
    lane = me % parts
    base = (me // group) * group
    local = me - base
    tokens, _ = qn_ref.shape
    rows, width = residual_ref.shape
    heads = len(ranges)
    head_width = q_send.shape[2]
    narrow_width = ranges[-1][0]
    broad_width = head_width - narrow_width
    span = 2 * tokens
    barrier = pltpu.get_barrier_semaphore()

    def remote(source, target, send, recv, sp, core):
        return pltpu.make_async_remote_copy(
            src_ref=source,
            dst_ref=target,
            send_sem=send,
            recv_sem=recv,
            device_id={"sp": sp, "tp": core},
            device_id_type=pl.DeviceIdType.MESH,
        )

    def flip(place, bit):
        return place + bit * (1 - 2 * ((place // bit) % 2))

    def mate(place, offset):
        bit = 1
        while bit <= offset:
            if offset & bit:
                place = flip(place, bit)
            bit *= 2
        return place

    def hello(k, carry):
        flat = (me * 2 + tp + k) % (count * 2)
        pl.semaphore_signal(
            barrier,
            inc=1,
            device_id={"sp": flat // 2, "tp": flat % 2},
            device_id_type=pl.DeviceIdType.MESH,
        )
        return carry

    lax.fori_loop(1, count * 2, hello, 0)

    def by_group(narrow_ref, broad_ref, h):
        return [
            narrow_ref[:, h * narrow_width : (h + 1) * narrow_width],
            broad_ref[:, h * broad_width : (h + 1) * broad_width],
        ]

    narrow_heads = heads - 1
    gates = jnp.concatenate([gn_ref[...], gb_ref[...]], axis=0)
    for h in range(head_groups):
        kv_send[h] = jnp.concatenate(
            by_group(kn_ref, kb_ref, h) + by_group(vn_ref, vb_ref, h), axis=1
        )
        q_send[h] = jnp.concatenate(by_group(qn_ref, qb_ref, h), axis=1)
        lines = []
        for i, (_, _, size) in enumerate(ranges):
            if i < narrow_heads:
                source = h * narrow_heads + i
            else:
                source = head_groups * narrow_heads + h
            lines += split_pieces(gates[source : source + 1] * size**0.5)
        lines += [jnp.ones((PIECES, tokens), jnp.float32)]
        gate_send[h] = pad_rows(jnp.concatenate(lines, axis=0), GATE_ROWS).astype(jnp.bfloat16)

    pl.semaphore_wait(barrier, count * 2 - 1)

    def line_copies(j, owner):
        target = (plane + j) % planes
        peer = target * parts + lane
        return (
            remote(
                kv_send.at[target], kv_all.at[owner], kv_line.at[0, j], kv_line.at[1, j], peer, tp
            ),
            remote(
                gate_send.at[target],
                gate_all.at[owner],
                gate_line.at[0, j],
                gate_line.at[1, j],
                peer,
                tp,
            ),
        )

    def line_owner(j):
        return ((plane + planes - j) % planes) * parts + lane

    def plane_copies(j, k, kv_source, gate_source, owner):
        peer = plane * parts + mate(lane, k)
        return (
            remote(
                kv_source,
                kv_all.at[owner],
                kv_plane.at[0, j, k],
                kv_plane.at[1, j, k],
                peer,
                tp,
            ),
            remote(
                gate_source,
                gate_all.at[owner],
                gate_plane.at[0, j, k],
                gate_plane.at[1, j, k],
                peer,
                tp,
            ),
        )

    for j in range(1, planes):
        for copy in line_copies(j, me):
            copy.start()
    for k in range(1, parts):
        for copy in plane_copies(0, k, kv_send.at[plane], gate_send.at[plane], me):
            copy.start()
    kv_all[me] = kv_send[plane]
    gate_all[me] = gate_send[plane]

    double = me // 2
    reader_part = jnp.where(double < parts, double, 2 * parts - 1 - double)
    my_slot = 2 * (double // parts) + me % 2

    def query_copies(h, slot, peer):
        return (
            remote(q_send.at[h], q_all.at[slot], q_sems.at[0, h], q_sems.at[1, slot], peer, tp),
            remote(
                gate_send.at[h],
                q_gate_all.at[slot],
                q_gate_sems.at[0, h],
                q_gate_sems.at[1, slot],
                peer,
                tp,
            ),
        )

    def tile_double(tile):
        return tile * (2 * parts - 1 - lane) + (1 - tile) * lane

    for h in range(head_groups):
        reader = h * parts + reader_part

        @pl.when(reader != me)
        def _():
            for copy in query_copies(h, my_slot, reader):
                copy.start()

        @pl.when(reader == me)
        def _():
            q_all[my_slot] = q_send[h]
            q_gate_all[my_slot] = gate_send[h]

    def project_pairs(h):
        pairs = []
        for source, low, size in (
            (pn_ref, 0, narrow_width),
            (pb_ref, narrow_width, broad_width),
        ):
            pairs.append(
                (
                    source.at[h * size : (h + 1) * size, :],
                    project.at[tp * head_groups + h, low : low + size, :],
                )
            )
        return pairs

    def project_copies(h):
        own, away = [], []
        for i, (source, target) in enumerate(project_pairs(h)):
            own.append(pltpu.make_async_copy(source, target, project_own.at[h, i]))
            away.append(
                remote(
                    source,
                    target,
                    project_sems.at[0, h, i],
                    project_sems.at[1, h, i],
                    me,
                    other,
                )
            )
        return own, away

    for h in range(head_groups):
        own, away = project_copies(h)
        for copy in own + away:
            copy.start()

    units = up_all.shape[2]

    def up_source(chunk):
        return up_ref.at[:, pl.ds(pl.multiple_of(chunk * units, 128), units)]

    def down_source(chunk):
        return down_ref.at[pl.ds(pl.multiple_of(chunk * units, units), units), :]

    def share_copy(which, offset, owner):
        peer = mate(local, offset)
        source = up_source(peer) if which == 0 else down_source(peer)
        target = up_all.at[owner] if which == 0 else down_all.at[owner]
        return remote(
            source,
            target,
            share_sems.at[0, which, offset],
            share_sems.at[1, which, offset],
            base + peer,
            tp,
        )

    twin = (me + group) % count
    twin_base = (base + group) % count

    def twin_copy(which, offset, index=None):
        index = offset if index is None else index
        owner = base + mate(local, offset)
        weights = up_all if which == 0 else down_all
        if offset:
            source = weights.at[owner]
        else:
            source = up_source(local) if which == 0 else down_source(local)
        return remote(
            source,
            weights.at[owner],
            twin_sems.at[0, which, index],
            twin_sems.at[1, which, index],
            twin,
            tp,
        )

    far = group // 2
    near = [offset for offset in range(1, group) if offset != far]
    near.sort(key=(1, 6, 5, 2, 3, 7).index)
    pieces = [(0, 0), (0, far), (1, 0), (1, far)] + [(0, offset) for offset in near]
    pieces += [(1, offset) for offset in (1, 2, 3, 6, 5, 7)]
    issued = []

    def tick(amount):
        for _ in range(amount):
            if len(issued) == len(pieces):
                return
            which, offset = pieces[len(issued)]
            if offset:
                share_copy(which, offset, base + mate(local, offset)).wait_recv()
            twin_copy(which, offset).start()
            issued.append((which, offset))

    own_weights = [
        pltpu.make_async_copy(up_source(local), up_all.at[me], own_sems.at[0]),
        pltpu.make_async_copy(down_source(local), down_all.at[me], own_sems.at[1]),
    ]
    for copy in own_weights:
        copy.start()
    for which in range(2):
        share_copy(which, far, me).start()
    tick(TICKS[0])

    for j in range(1, planes):
        owner = line_owner(j)
        for copy in line_copies(j, owner):
            copy.wait_recv()
        for k in range(1, parts):
            for copy in plane_copies(j, k, kv_all.at[owner], gate_all.at[owner], owner):
                copy.start()

    for offset in near:
        share_copy(0, offset, me).start()
    tick(TICKS[1])

    for slot in range(4):
        owner = 2 * tile_double(slot // 2) + slot % 2

        @pl.when(owner != me)
        def _():
            for copy in query_copies(0, slot, owner):
                copy.wait_recv()

    lane_id = lax.broadcasted_iota(jnp.int32, (span, head_width), 1)
    first_one = heads * PIECES

    def turned_gates(lines):
        block = pad_lanes(pad_rows(lines.astype(jnp.float32), 128), -(-tokens // 128) * 128)
        return block.T[:tokens]

    def widen(tile, carry):
        query = q_all[pl.ds(2 * tile, 2)].reshape(span, head_width).astype(jnp.float32)
        own_gates = jnp.concatenate(
            [turned_gates(q_gate_all[2 * tile + i]) for i in range(2)], axis=0
        )
        for i, (low, high, _) in enumerate(ranges):
            left = jnp.where((lane_id >= low) & (lane_id < high), query, 0.0)
            moved = pltpu.roll(own_gates, first_one - i * PIECES, 1)
            right = jnp.where((lane_id >= first_one) & (lane_id < first_one + PIECES), moved, 0.0)
            right = jnp.where(
                (lane_id >= i * PIECES) & (lane_id < (i + 1) * PIECES), -1.0, right
            )
            q_wide[tile, i] = jnp.concatenate([left, right], axis=1).astype(jnp.bfloat16)
        acc[tile] = jnp.zeros((head_width, span), jnp.float32)
        peaks[tile] = jnp.full((heads, 1, span), -1e30, jnp.float32)
        totals[tile] = jnp.zeros((heads, 1, span), jnp.float32)
        return carry

    lax.fori_loop(0, 2, widen, 0)

    def turn(pair):
        values = kv_all[pl.ds(2 * pair, 2), :, head_width:].reshape(span, head_width)
        v_turned[pair] = values.astype(jnp.float32).T.astype(jnp.bfloat16)
        for i in range(2):
            key_gates[2 * pair + i] = turned_gates(gate_all[2 * pair + i]).astype(jnp.bfloat16)

    def attend(tile, pair, masked):
        keys = jnp.concatenate(
            [
                kv_all[pl.ds(2 * pair, 2), :, :head_width].reshape(span, head_width),
                key_gates[pl.ds(2 * pair, 2)].reshape(span, head_width),
            ],
            axis=1,
        )
        for i, (low, high, size) in enumerate(ranges):
            factor = size**-0.5 * LOG2E
            scores = lax.dot_general(
                keys, q_wide[tile, i], (((1,), (1,)), ((), ())), preferred_element_type=jnp.float32
            )
            if masked:
                row = lax.broadcasted_iota(jnp.int32, (span, span), 0)
                column = lax.broadcasted_iota(jnp.int32, (span, span), 1)
                scores = jnp.where(row <= column, scores, -1e30)
            before = peaks[tile, i]
            peak = jnp.maximum(before, jnp.max(scores, axis=0, keepdims=True))
            weights = jnp.exp2((scores - peak) * factor)
            fade = jnp.exp2((before - peak) * factor)
            peaks[tile, i] = peak
            totals[tile, i] = totals[tile, i] * fade + jnp.sum(weights, axis=0, keepdims=True)
            acc[tile, low:high, :] = acc[tile, low:high, :] * fade + jnp.dot(
                v_turned[pair, low:high, :],
                weights.astype(jnp.bfloat16),
                preferred_element_type=jnp.float32,
            )

    for j in range(planes):
        source_plane = (plane + planes - j) % planes
        for k in range(1, parts):
            owner = source_plane * parts + mate(lane, k)
            for copy in plane_copies(j, k, kv_all.at[owner], gate_all.at[owner], owner):
                copy.wait_recv()

        def visit(i, carry):
            pair = source_plane * (parts // 2) + i // 2
            tile = i % 2
            double_block = tile_double(tile)

            @pl.when(tile == 0)
            def _():
                turn(pair)

            @pl.when(pair < double_block)
            def _():
                attend(tile, pair, False)

            @pl.when(pair == double_block)
            def _():
                attend(tile, pair, True)

            return carry

        lax.fori_loop(0, parts, visit, 0)
        tick(TICKS[2 + j])

    def settle(tile, carry):
        scaled = jnp.concatenate(
            [acc[tile, low:high, :] / totals[tile, i] for i, (low, high, _) in enumerate(ranges)],
            axis=0,
        )
        attended[pl.ds(2 * tile, 2)] = (
            scaled.T.astype(jnp.bfloat16).reshape(2, tokens, head_width)
        )
        return carry

    lax.fori_loop(0, 2, settle, 0)

    def back_copy(slot, core, place, sp):
        return remote(
            attended.at[slot, core * rows : (core + 1) * rows, :],
            attended_in.at[place],
            back_sems.at[0, slot, core],
            back_sems.at[1, 0, place],
            sp,
            core,
        )

    my_place = tp * head_groups + plane
    for slot in range(4):
        owner = 2 * tile_double(slot // 2) + slot % 2
        for core in range(2):
            here = (owner == me) & (tp == core)

            @pl.when(jnp.logical_not(here))
            def _():
                back_copy(slot, core, my_place, owner).start()

            @pl.when(here)
            def _():
                attended_in[my_place] = attended[slot, core * rows : (core + 1) * rows, :]

    for offset in (1, 2, 3, 6, 5, 7):
        share_copy(1, offset, me).start()
    tick(TICKS[6])
    for h in range(head_groups):
        own, away = project_copies(h)
        for copy in own:
            copy.wait()
        for copy in away:
            copy.wait()
    for h in range(head_groups):
        for core in range(2):
            place = core * head_groups + h
            sender = h * parts + reader_part

            @pl.when(jnp.logical_not((sender == me) & (tp == core)))
            def _():
                remote(
                    attended.at[0, :rows, :],
                    attended_in.at[place],
                    back_sems.at[0, 0, 0],
                    back_sems.at[1, 0, place],
                    sender,
                    core,
                ).wait_recv()

    step_width = return_out.shape[3]
    chunks = width // step_width
    joined = jnp.concatenate([attended_in[i] for i in range(2 * head_groups)], axis=1)

    def project_step(n, squares):
        columns = pl.ds(pl.multiple_of(n * step_width, step_width), step_width)
        total = residual_ref[:, columns].astype(jnp.float32) + jnp.dot(
            joined,
            project[:, :, columns].reshape(2 * head_groups * head_width, step_width),
            preferred_element_type=jnp.float32,
        )
        total = total.astype(jnp.bfloat16).astype(jnp.float32)
        mixed[:, columns] = total
        return squares + jnp.sum(total * total, axis=1, keepdims=True)

    tick(TICKS[7])
    squares = lax.fori_loop(0, chunks, project_step, jnp.zeros((rows, 1), jnp.float32))
    scale = lax.rsqrt(squares / width + 1e-06)
    scaled_rows = (mixed[...] * scale * gain_ref[...]).astype(jnp.bfloat16)
    normed[...] = scaled_rows
    features[tp, local] = scaled_rows

    bits = (group // 2, 1 + tp, 2 - tp)
    levels = len(bits)

    def member(subset):
        place = local
        for level in range(levels):
            if (subset >> level) & 1:
                place = flip(place, bits[level])
        return place

    def across(subset):
        level = subset.bit_length() - 1
        held = subset - (1 << level)
        owner = member(held)
        return remote(
            features.at[tp, owner] if held else normed,
            features.at[tp, owner],
            across_sems.at[0, subset],
            across_sems.at[1, subset],
            base + flip(local, bits[level]),
            tp,
        )

    def beside(subset):
        owner = member(subset)
        return remote(
            features.at[tp, owner] if subset else normed,
            features.at[tp, owner],
            beside_sems.at[0, subset],
            beside_sems.at[1, subset],
            me,
            other,
        )

    def spread(subset):
        for level in range(subset.bit_length(), levels):
            across(subset + (1 << level)).start()
        beside(subset).start()

    spread(0)
    tick(TICKS[8])
    for subset in (2, 1, 3):
        across(subset).wait_recv()
        spread(subset)
        tick(TICKS[9])
    tick(len(pieces))
    own_weights[0].wait()
    row_groups = 2
    some = group // row_groups

    def up_step(core, place):
        chips = pl.ds(place * some, some)
        total = jnp.dot(
            features[core, chips].reshape(some * rows, width),
            up_all[...].reshape(width, units),
            preferred_element_type=jnp.float32,
        )
        total = jnp.maximum(total, 0.0)
        hidden[core, chips] = (
            (total * total).astype(jnp.bfloat16).reshape(some, rows, units)
        )

    home = local // some
    for subset in (4, 6):
        across(subset).wait_recv()
        spread(subset)
    for subset in (0, 2, 4, 6):
        beside(subset).wait_recv()
    for offset in range(group):
        twin_copy(0, offset).wait_recv()

    def up_both(place):
        def inner(core, carry):
            up_step(core, place)
            return carry

        lax.fori_loop(0, 2, inner, 0)

    up_both(home)
    for subset in (5, 7):
        across(subset).wait_recv()
        spread(subset)
    for subset in (1, 3, 5, 7):
        beside(subset).wait_recv()
    up_both(1 - home)
    own_weights[1].wait()
    per_chunk = count // chunks

    def chunk_of(i):
        return ((base + (i // 2) * group) % count) // per_chunk + (local // per_chunk + i) % 2

    def wait_down(i):
        if i >= chunks // 2:
            for k in range(per_chunk):
                twin_copy(1, (i % 2) * per_chunk + k).wait_recv()

    def down_columns(chunk):
        return jnp.concatenate(
            [down_all[chunk * per_chunk + i] for i in range(per_chunk)], axis=1
        )

    def part_copy(chunk):
        return remote(
            part_out.at[chunk],
            part_in.at[chunk],
            part_sems.at[0, chunk],
            part_sems.at[1, chunk],
            me,
            other,
        )

    def down_dot(core, chips, chunk):
        return jnp.dot(
            hidden[core, chips].reshape(some * rows, units),
            down_columns(chunk),
            preferred_element_type=jnp.float32,
        ).reshape(some, rows, step_width)

    def away_step(chunk):
        def inner(i, carry):
            chips = pl.ds(i * some, some)
            part_out[chunk, chips] = down_dot(other, chips, chunk).astype(jnp.bfloat16)
            return carry

        lax.fori_loop(0, row_groups, inner, 0)
        part_copy(chunk).start()


    def return_copy(chunk, subset):
        level = subset.bit_length() - 1
        return remote(
            return_out.at[chunk, member(subset)],
            return_in.at[chunk, subset],
            return_sems.at[0, chunk, subset],
            return_sems.at[1, chunk, subset],
            base + flip(local, bits[level]),
            tp,
        )

    def home_step(chunk):
        part_copy(chunk).wait_recv()

        def inner(i, carry):
            chips = pl.ds(i * some, some)
            return_out[chunk, chips] = (
                down_dot(tp, chips, chunk) + part_in[chunk, chips].astype(jnp.float32)
            ).astype(jnp.bfloat16)
            return carry

        lax.fori_loop(0, row_groups, inner, 0)
        for subset in range(group // 2, group):
            return_copy(chunk, subset).start()

    wait_down(0)
    away_step(chunk_of(0))
    for i in range(chunks):
        if i + 1 < chunks:
            wait_down(i + 1)
            away_step(chunk_of(i + 1))
        home_step(chunk_of(i))

    for level in range(levels - 1, 0, -1):

        def merge_step(i, carry):
            chunk = chunk_of(i)
            for held in range(1 << level):
                return_copy(chunk, held + (1 << level)).wait_recv()
                place = member(held)
                return_out[chunk, place] = (
                    return_out[chunk, place].astype(jnp.float32)
                    + return_in[chunk, held + (1 << level)].astype(jnp.float32)
                ).astype(jnp.bfloat16)
            for subset in range(1 << (level - 1), 1 << level):
                return_copy(chunk, subset).start()
            return carry

        lax.fori_loop(0, chunks, merge_step, 0)

    def final_step(i, carry):
        chunk = chunk_of(i)
        columns = pl.ds(pl.multiple_of(chunk * step_width, step_width), step_width)
        return_copy(chunk, 1).wait_recv()
        total = (
            mixed[:, columns]
            + return_out[chunk, local].astype(jnp.float32)
            + return_in[chunk, 1].astype(jnp.float32)
        )
        out_ref[:, columns] = total.astype(jnp.bfloat16)
        return carry

    lax.fori_loop(0, chunks, final_step, 0)

    for j in range(1, planes):
        for copy in line_copies(j, me):
            copy.wait_send()
    for j in range(planes):
        for k in range(1, parts):
            for copy in plane_copies(j, k, kv_send.at[plane], gate_send.at[plane], me):
                copy.wait_send()
    for h in range(head_groups):
        reader = h * parts + reader_part

        @pl.when(reader != me)
        def _():
            for copy in query_copies(h, my_slot, reader):
                copy.wait_send()

    for slot in range(4):
        owner = 2 * tile_double(slot // 2) + slot % 2
        for core in range(2):
            here = (owner == me) & (tp == core)

            @pl.when(jnp.logical_not(here))
            def _():
                back_copy(slot, core, my_place, owner).wait_send()

    for which in range(2):
        for offset in range(1, group):
            share_copy(which, offset, me).wait_send()
    for which, offset in pieces:
        twin_copy(which, offset).wait_send()
    for subset in range(group):
        if subset:
            across(subset).wait_send()
        beside(subset).wait_send()

    def returns_sent(chunk, carry):
        part_copy(chunk).wait_send()
        for subset in range(1, group):
            return_copy(chunk, subset).wait_send()
        return carry

    lax.fori_loop(0, chunks, returns_sent, 0)


def fused_local(
    residual,
    queries_narrow,
    keys_narrow,
    values_narrow,
    queries_broad,
    keys_broad,
    values_broad,
    gates_narrow,
    gates_broad,
    project_narrow,
    project_broad,
    norm_gain,
    up_weight,
    down_weight,
):
    count = lax.axis_size("sp")
    group = group_size(count)
    tokens = queries_narrow.shape[0]
    rows, width = residual.shape
    head_groups = gates_broad.shape[1]
    parts = count // head_groups
    narrow_heads = gates_narrow.shape[1] // head_groups
    ranges = head_columns(narrow_heads)
    heads = len(ranges)
    head_width = ranges[-1][1]
    up_rows, unit_total = up_weight.shape
    units = unit_total // group
    columns = down_weight.shape[1]
    step_width = 4 * columns
    chunks = width // step_width
    span = 2 * tokens
    kind = residual.dtype
    vmem = pl.BlockSpec(memory_space=pltpu.VMEM)
    anywhere = pl.BlockSpec(memory_space=pl.ANY)
    dma = pltpu.SemaphoreType.DMA
    returned = (chunks, group, rows, step_width)
    return pl.pallas_call(
        functools.partial(fused_kernel, count, group, head_groups, ranges),
        out_shape=jax.ShapeDtypeStruct(residual.shape, kind),
        in_specs=[vmem] * 10 + [anywhere] * 4,
        out_specs=vmem,
        scratch_shapes=[
            pltpu.VMEM((head_groups, tokens, head_width), kind),
            pltpu.VMEM((head_groups, tokens, 2 * head_width), kind),
            pltpu.VMEM((head_groups, GATE_ROWS, tokens), kind),
            pltpu.VMEM((4, tokens, head_width), kind),
            pltpu.VMEM((4, GATE_ROWS, tokens), kind),
            pltpu.VMEM((count, tokens, 2 * head_width), kind),
            pltpu.VMEM((count, GATE_ROWS, tokens), kind),
            pltpu.VMEM((count, tokens, head_width), kind),
            pltpu.VMEM((count // 2, head_width, span), kind),
            pltpu.VMEM((2, heads, span, 2 * head_width), kind),
            pltpu.VMEM((2, head_width, span), jnp.float32),
            pltpu.VMEM((2, heads, 1, span), jnp.float32),
            pltpu.VMEM((2, heads, 1, span), jnp.float32),
            pltpu.VMEM((4, tokens, head_width), kind),
            pltpu.VMEM((2 * head_groups, rows, head_width), kind),
            pltpu.VMEM((2 * head_groups, head_width, width), kind),
            pltpu.VMEM((rows, width), jnp.float32),
            pltpu.VMEM((rows, width), kind),
            pltpu.VMEM((count, up_rows, units), kind),
            pltpu.VMEM((count, units, columns), kind),
            pltpu.VMEM((2, group, rows, width), kind),
            pltpu.VMEM((2, group, rows, units), kind),
            pltpu.VMEM(returned, kind),
            pltpu.VMEM(returned, kind),
            pltpu.VMEM(returned, kind),
            pltpu.VMEM(returned, kind),
            dma((2, head_groups)),
            dma((2, head_groups)),
            dma((2, head_groups, parts)),
            dma((2, head_groups, parts)),
            dma((2, 4)),
            dma((2, 4)),
            dma((2, 4, 2 * head_groups)),
            dma((head_groups, 2)),
            dma((2, head_groups, 2)),
            dma((2, 2, group)),
            dma((2, 2, group)),
            dma((2,)),
            dma((2, group)),
            dma((2, group)),
            dma((2, chunks)),
            dma((2, chunks, group)),
        ],
        compiler_params=pltpu.CompilerParams(
            collective_id=3, has_side_effects=True, vmem_limit_bytes=60 * 2**20
        ),
    )(
        residual,
        queries_narrow,
        keys_narrow,
        values_narrow,
        queries_broad,
        keys_broad,
        values_broad,
        gates_narrow.T,
        gates_broad.T,
        norm_gain.reshape(1, -1),
        project_narrow,
        project_broad,
        up_weight,
        down_weight,
    )


def layer(*arrays):
    queries, gates_broad, down_weight = arrays[1], arrays[8], arrays[13]
    head_groups = gates_broad.shape[1]
    narrow_heads = arrays[7].shape[1] // head_groups
    fused = (
        lax.axis_size("tp") == 2
        and head_groups == 4
        and lax.axis_size("sp") == head_groups * 4
        and group_size(lax.axis_size("sp")) == 8
        and narrow_heads * A_DIM + B_DIM == 128
        and down_weight.shape[1] % 128 == 0
        and queries.shape[0] % 64 == 0
    )
    return fused_local(*arrays) if fused else local(*arrays)


def solution(mesh):
    return jax.shard_map(
        layer,
        mesh=mesh,
        in_specs=(
            P(("sp", "tp"), None),
            P("sp", "tp"),
            P("sp", "tp"),
            P("sp", "tp"),
            P("sp", "tp"),
            P("sp", "tp"),
            P("sp", "tp"),
            P("sp", "tp"),
            P("sp", "tp"),
            P("tp", None),
            P("tp", None),
            P(),
            P("sp", "tp"),
            P("tp", "sp"),
        ),
        out_specs=P(("sp", "tp"), None),
        check_vma=False,
    )
```
